512 devices in a mesh: grp: 2 (over y), kv: 32 (over z), tp: 8 (over x, core).
Axes of the slice: x: 4, y: 2, z: 32, core: 2. Of those that a mesh axis runs over, the one named last changes fastest.
The devices are a block of a 4x8x32 slice.
Arguments:
- tokens: bfloat16 [256, 4096], P('grp', 'kv'), parts along dimension 0, may hold values from -40 to 40
- lengths: int32 [256], P(('grp', 'kv')), parts along dimension 0, may hold values from 1 to 6, 320 in all
- conv_state_x: bfloat16 [256, 3, 4096], P(('grp', 'kv'), None, 'tp'), parts along dimension 0, may hold values from -6 to 6
- conv_state_bc: bfloat16 [256, 3, 2, 1024], P(('grp', 'kv'), None, None, 'tp'), parts along dimension 0, may hold values from -6 to 6
- ssm_state: float32 [256, 64, 64, 128], P(('grp', 'kv'), 'tp'), parts along dimension 0, may hold values from -0.6 to 0.6
- norm_gain: bfloat16 [4096], P('kv'), may hold values from 0.099609375 to 1.8984375
- w_gate: bfloat16 [4096, 4096], P('kv', 'tp'), may hold values from -0.09375 to 0.09375
- w_value: bfloat16 [4096, 4096], P('kv', 'tp'), may hold values from -0.09375 to 0.09375
- w_key: bfloat16 [4096, 1024], P('kv', 'tp'), may hold values from -0.09375 to 0.09375
- w_query: bfloat16 [4096, 1024], P('kv', 'tp'), may hold values from -0.09375 to 0.09375
- w_step: bfloat16 [4096, 64], P('kv', 'tp'), may hold values from -0.09375 to 0.09375
- step_bias: float32 [64], P('tp'), may hold values from -2 to 0
- decay_log: float32 [64], P('tp'), may hold values from -2 to 1
- conv_x: bfloat16 [4, 4096], P(None, 'tp'), may hold values from -3 to 3
- conv_bc: bfloat16 [4, 2, 1024], P(None, None, 'tp'), may hold values from -3 to 3
- inner_gain: bfloat16 [4096], P('tp'), may hold values from 0.099609375 to 1.8984375
- w_out: bfloat16 [4096, 4096], P('tp', 'kv'), may hold values from -0.09375 to 0.09375
- mlp_gain: bfloat16 [4096], P('kv'), may hold values from 0.099609375 to 1.8984375
- w_up: bfloat16 [4096, 16384], P('kv', 'tp'), may hold values from -0.09375 to 0.09375
- w_down: bfloat16 [16384, 4096], P('tp', 'kv'), may hold values from -0.046875 to 0.046875
Outputs:
- layer_out: bfloat16 [256, 4096], P('grp', 'kv'), parts along dimension 0
- next_state: float32 [256, 64, 64, 128], P(('grp', 'kv'), 'tp'), parts along dimension 0
The draws below stay inside these ranges and needn't reach their ends.
There are 2 independent parts, one for each index of `grp`. The reference program is written for one: setup_inputs(seed, part) draws one part's arguments, and reference() takes and returns one part's arrays. A program takes and returns all parts, laid end to end along the dimension named above; an argument that names none is the same for every part. Nothing has to cross between parts.
All inputs are finite; a program needn't handle non-finite values. No bound on the sum of `lengths` on one device may be relied on, other than what follows from the above.
Results may differ from the reference program's by a relative error of at most 0.008.
Values may be sent and summed in bfloat16 or wider, within the bound.
No kernel may reach another device: no remote copies, remote signals or barrier semaphores. Data moves between devices by JAX's collectives and lax.ppermute only.
A program may use at most 64 MiB of HBM per device.

```python
import math
import jax
import jax.numpy as jnp
import numpy as np
from jax import lax

D = 4096
HEADS = 64
HEAD_DIM = 64
GROUPS = 8
STATE = 128
FF = 16384
CONV_WIDTH = 4
INNER = 4096
BATCH = 128


def draw_tokens(key, part):
    base_key = jax.random.fold_in(jax.random.fold_in(key, 11), 0)
    columns = jnp.arange(D, dtype=jnp.float32) / D
    col_scale = 0.6 * jnp.exp(jnp.log(4.0) * columns)[None, :]
    base_draw = jnp.clip(jax.random.normal(base_key, (BATCH, D), jnp.float32), -6.0, 6.0)
    return (base_draw * col_scale).astype(jnp.bfloat16)


def steps_of(stream_key, shape, cuts, smallest, largest):
    factor_of = 1.0
    for position, shards_of in cuts:
        heights = jax.random.uniform(jax.random.fold_in(jax.random.fold_in(stream_key, 6), position), (shards_of,), jnp.float32, smallest / len(cuts), largest / len(cuts))
        factor_of = factor_of * jnp.repeat(jnp.exp(heights), shape[position] // shards_of).reshape((-1,) + (1,) * (len(shape) - 1 - position))
    return factor_of


def profile(number_of, total, reach, slope):
    portions = [(1 << 20) // math.isqrt(standing ** slope) + 1 for standing in range(2, number_of + 1)]
    rest, holding = total - reach - (number_of - 1), [1] * (number_of - 1)
    while rest > 0:
        candidates = [i for i in range(number_of - 1) if holding[i] < reach]
        pool, left = sum([portions[i] for i in candidates]), rest
        for i in candidates:
            addition = min(reach - holding[i], max(1, left * portions[i] // pool), rest)
            holding[i] = holding[i] + addition
            rest = rest - addition
    return np.array([reach] + holding)


def uneven(stream_key, number_of, total, limit, lean):
    if number_of == 2:
        one = jax.random.randint(stream_key, (), max(1, total - limit), min(limit, total - 1) + 1)
        return jnp.stack([one, total - one])
    tallies = jnp.asarray(profile(number_of, total, limit, lean), jnp.int32)
    twos = (number_of - 1) // 2
    source_of, taker = tallies[1:1 + 2 * twos:2], tallies[2:2 + 2 * twos:2]
    room = jnp.minimum(source_of - 1, limit - taker)
    passed = jax.random.randint(jax.random.fold_in(stream_key, 1), (twos,), 0, 1 << 20) % (room + 1)
    tallies = tallies.at[1:1 + 2 * twos:2].set(source_of - passed).at[2:2 + 2 * twos:2].set(taker + passed)
    return tallies[jax.random.permutation(jax.random.fold_in(stream_key, 2), number_of)]


def centred(key, extent, scale, reach, shards=(), held_as=jnp.bfloat16):
    drawn = scale * jax.random.normal(key, extent, jnp.float32)
    if shards:
        drawn = drawn * steps_of(key, extent, shards, -0.22, 0.18)
    return jnp.clip(drawn, -reach, reach).astype(held_as)


def setup_inputs(seed: int = 0, part: int = 0) -> dict:
    key_list = jax.random.split(jax.random.key(seed), 21)
    own_keys = jax.random.split(jax.random.fold_in(key_list[20], part), 21)
    return {
        "tokens": draw_tokens(jax.random.fold_in(jax.random.fold_in(key_list[20], part), 71), part),
        "lengths": uneven(own_keys[1], BATCH, BATCH * 5 // 2, 6, 2).astype(jnp.int32),
        "conv_state_x": centred(own_keys[2], (BATCH, CONV_WIDTH - 1, INNER), 1.0, 6.0, ((0, 32), (2, 8))),
        "conv_state_bc": centred(own_keys[3], (BATCH, CONV_WIDTH - 1, 2, GROUPS * STATE), 1.0, 6.0, ((0, 32), (3, 8))),
        "ssm_state": centred(own_keys[4], (BATCH, HEADS, HEAD_DIM, STATE), 0.1, 0.6, ((0, 32), (1, 8)), jnp.float32),
        "norm_gain": jnp.clip(1.0 + 0.18 * jax.random.normal(key_list[5], (D,), jnp.float32), 0.099609375, 1.8984375).astype(jnp.bfloat16),
        "w_gate": centred(key_list[6], (D, INNER), D ** -0.5, 0.09375, ((0, 32), (1, 8))),
        "w_value": centred(key_list[7], (D, INNER), D ** -0.5, 0.09375, ((0, 32), (1, 8))),
        "w_key": centred(key_list[8], (D, GROUPS * STATE), D ** -0.5, 0.09375, ((0, 32), (1, 8))),
        "w_query": centred(key_list[9], (D, GROUPS * STATE), D ** -0.5, 0.09375, ((0, 32), (1, 8))),
        "w_step": centred(key_list[10], (D, HEADS), D ** -0.5, 0.09375, ((0, 32), (1, 8))),
        "step_bias": jnp.clip(-2.0 + 2.0 * jax.random.uniform(key_list[11], (HEADS,), jnp.float32) ** steps_of(key_list[11], (HEADS,), ((0, 8),), -0.2, 0.2), -2.0, 0.0),
        "decay_log": jnp.clip(-2.0 + 3.0 * jax.random.uniform(key_list[12], (HEADS,), jnp.float32) ** steps_of(key_list[12], (HEADS,), ((0, 8),), -0.2, 0.2), -2.0, 1.0),
        "conv_x": centred(key_list[13], (CONV_WIDTH, INNER), CONV_WIDTH ** -0.5, 3.0, ((1, 8),)),
        "conv_bc": centred(key_list[14], (CONV_WIDTH, 2, GROUPS * STATE), CONV_WIDTH ** -0.5, 3.0, ((2, 8),)),
        "inner_gain": jnp.clip(1.0 + 0.18 * jax.random.normal(key_list[15], (INNER,), jnp.float32), 0.099609375, 1.8984375).astype(jnp.bfloat16),
        "w_out": centred(key_list[16], (INNER, D), INNER ** -0.5, 0.09375, ((0, 8), (1, 32))),
        "mlp_gain": jnp.clip(1.0 + 0.18 * jax.random.normal(key_list[17], (D,), jnp.float32), 0.099609375, 1.8984375).astype(jnp.bfloat16),
        "w_up": centred(key_list[18], (D, FF), D ** -0.5, 0.09375, ((0, 32), (1, 8))),
        "w_down": centred(key_list[19], (FF, D), FF ** -0.5, 0.046875, ((0, 8), (1, 32))),
    }


epsilon = 1e-06

def causal_conv(state_rows, newest, conv_weights):
    extended = jnp.concatenate([state_rows, newest[:, None]], axis=1)
    conv_sum = extended[:, 0] * conv_weights[0].astype(jnp.float32)
    for offset in range(1, conv_weights.shape[0]):
        conv_sum = conv_sum + extended[:, offset] * conv_weights[offset].astype(jnp.float32)
    return jax.nn.silu(conv_sum)

def product(left, right):
    return jnp.dot(left, right, preferred_element_type=jnp.float32)

def reference(tokens, lengths, conv_state_x, conv_state_bc, ssm_state, norm_gain, w_gate, w_value, w_key, w_query, w_step, step_bias, decay_log, conv_x, conv_bc, inner_gain, w_out, mlp_gain, w_up, w_down):
    seq_count = tokens.shape[0]
    per_group = HEADS // GROUPS
    widened = tokens.astype(jnp.float32)
    inverse = lax.rsqrt(lax.optimization_barrier(jnp.mean(widened * widened, axis=1, keepdims=True)) + epsilon)
    scaled = (widened * norm_gain.astype(jnp.float32)).astype(jnp.bfloat16)
    gate_pre = product(scaled, w_gate) * inverse
    value_pre = product(scaled, w_value) * inverse
    key_pre = product(scaled, w_key) * inverse
    query_pre = product(scaled, w_query) * inverse
    step_pre = product(scaled, w_step) * inverse
    row_live = (jnp.arange(CONV_WIDTH - 1, dtype=jnp.int32)[None, :] >= CONV_WIDTH - 1 - lengths[:, None]).astype(jnp.float32)
    live_x = conv_state_x.astype(jnp.float32) * row_live[:, :, None]
    live_bc = conv_state_bc.astype(jnp.float32) * row_live[:, :, None, None]
    mixed_values = causal_conv(live_x, value_pre, conv_x).reshape(seq_count, HEADS, HEAD_DIM)
    key_query = causal_conv(live_bc, jnp.stack([key_pre, query_pre], axis=1), conv_bc)
    key_heads = jnp.repeat(key_query[:, 0].reshape(seq_count, GROUPS, STATE), per_group, axis=1)
    query_heads = jnp.repeat(key_query[:, 1].reshape(seq_count, GROUPS, STATE), per_group, axis=1)
    step_size = jax.nn.softplus(step_pre + step_bias)
    rate_now = -jnp.exp(decay_log) * step_size
    next_state = ssm_state * jnp.exp(rate_now)[:, :, None, None] + (step_size[:, :, None] * mixed_values)[:, :, :, None] * key_heads[:, :, None, :]
    mixer_y = jnp.einsum('bhpn,bhn->bhp', next_state, query_heads, precision=lax.Precision.HIGHEST).reshape(seq_count, INNER)
    gated_rows = mixer_y * jax.nn.silu(gate_pre)
    gated_inverse = lax.rsqrt(lax.optimization_barrier(jnp.mean(gated_rows * gated_rows, axis=1, keepdims=True)) + epsilon)
    gated_low = (gated_rows * inner_gain.astype(jnp.float32)).astype(jnp.bfloat16)
    residual = (widened + product(gated_low, w_out) * gated_inverse).astype(jnp.bfloat16)
    residual_wide = residual.astype(jnp.float32)
    residual_inverse = lax.rsqrt(lax.optimization_barrier(jnp.mean(residual_wide * residual_wide, axis=1, keepdims=True)) + epsilon)
    hidden_low = (residual_wide * mlp_gain.astype(jnp.float32)).astype(jnp.bfloat16)
    activation = jnp.square(jax.nn.relu(product(hidden_low, w_up) * residual_inverse)).astype(jnp.bfloat16)
    layer_out = (residual_wide + product(activation, w_down)).astype(jnp.bfloat16)
    return (layer_out, next_state)
```

```python
import jax
import jax.numpy as jnp
from jax import lax
from jax.sharding import Mesh, PartitionSpec as P

HEAD_DIM = 64
STATE = 128
CONV_WIDTH = 4
LANES = 128
NEAR = 4

epsilon = 1e-06
f32, bf16 = jnp.float32, jnp.bfloat16


def scattered_sum(rows, along):
    size = lax.axis_size(along)
    parts = rows.reshape(size, -1, rows.shape[1])
    return lax.all_to_all(parts, along, 0, 0, tiled=True).astype(f32).sum(axis=0)


def from_everyone(shard, along):
    copies = jnp.broadcast_to(shard, (lax.axis_size(along), *shard.shape))
    return lax.all_to_all(copies, along, 0, 0, tiled=True)


def hi_lo(column):
    hi = column.astype(bf16)
    lo = (column - hi.astype(f32)).astype(bf16)
    lane = lax.broadcasted_iota(jnp.int32, (column.shape[0], LANES), 1)
    return jnp.where(lane == 0, hi, jnp.where(lane == 1, lo, jnp.zeros((), bf16)))


def causal_conv(state_rows, newest, conv_weights):
    extended = jnp.concatenate([state_rows, newest[:, None]], axis=1)
    conv_sum = extended[:, 0] * conv_weights[0].astype(f32)
    for offset in range(1, conv_weights.shape[0]):
        conv_sum = conv_sum + extended[:, offset] * conv_weights[offset].astype(f32)
    return jax.nn.silu(conv_sum)


def product(left, right, out=f32):
    return jnp.dot(left, right, preferred_element_type=out)


def per_device(
    tokens,
    lengths,
    conv_state_x,
    conv_state_bc,
    ssm_state,
    norm_gain,
    w_gate,
    w_value,
    w_key,
    w_query,
    w_step,
    step_bias,
    decay_log,
    conv_x,
    conv_bc,
    inner_gain,
    w_out,
    mlp_gain,
    w_up,
    w_down,
):
    far, near = lax.axis_size("far"), lax.axis_size("near")
    kv = ("far", "near")
    head_count = w_step.shape[1]
    group_count = w_key.shape[1] // STATE
    per_group = head_count // group_count
    batch, width = tokens.shape
    model = width * far * near
    inner = w_gate.shape[1] * lax.axis_size("tp")
    seqs = batch // (far * near)

    ordered = tokens.reshape(far, near, seqs, width).swapaxes(0, 1).reshape(batch, width)
    wide = ordered.astype(f32)
    scaled = (wide * norm_gain.astype(f32)).astype(bf16)
    partial = jnp.concatenate(
        [
            product(scaled, w_gate, bf16),
            product(scaled, w_value, bf16),
            product(scaled, w_key, bf16),
            product(scaled, w_query, bf16),
            product(scaled, w_step, bf16),
            hi_lo(jnp.sum(wide * wide, axis=1, keepdims=True))[:, : LANES - head_count],
        ],
        axis=1,
    )
    mine = scattered_sum(scattered_sum(partial, "near").astype(bf16), "far")
    cuts, at = [], 0
    for size in (w_gate.shape[1], w_value.shape[1], w_key.shape[1], w_query.shape[1], head_count):
        cuts.append(mine[:, at : at + size])
        at += size
    gate_raw, value_raw, key_raw, query_raw, step_raw = cuts
    squares = jnp.sum(mine[:, at:], axis=1, keepdims=True)
    inverse = lax.rsqrt(squares / model + epsilon)

    row_live = (
        jnp.arange(CONV_WIDTH - 1, dtype=jnp.int32)[None, :] >= CONV_WIDTH - 1 - lengths[:, None]
    ).astype(f32)
    live_x = conv_state_x.astype(f32) * row_live[:, :, None]
    live_bc = conv_state_bc.astype(f32) * row_live[:, :, None, None]
    mixed_values = causal_conv(live_x, value_raw * inverse, conv_x).reshape(
        seqs, head_count, HEAD_DIM
    )
    key_query = causal_conv(
        live_bc, jnp.stack([key_raw * inverse, query_raw * inverse], axis=1), conv_bc
    )
    key_heads = jnp.repeat(key_query[:, 0].reshape(seqs, group_count, STATE), per_group, axis=1)
    query_heads = jnp.repeat(key_query[:, 1].reshape(seqs, group_count, STATE), per_group, axis=1)
    step_size = jax.nn.softplus(step_raw * inverse + step_bias)
    rate_now = -jnp.exp(decay_log) * step_size
    next_state = (
        ssm_state * jnp.exp(rate_now)[:, :, None, None]
        + (step_size[:, :, None] * mixed_values)[:, :, :, None] * key_heads[:, :, None, :]
    )
    mixer_y = jnp.sum(next_state * query_heads[:, :, None, :], axis=3).reshape(
        seqs, head_count * HEAD_DIM
    )
    gated_rows = mixer_y * jax.nn.silu(gate_raw * inverse)
    gated_low = (gated_rows * inner_gain.astype(f32)).astype(bf16)

    all_low = from_everyone(gated_low, kv).reshape(batch, -1)
    ungained = all_low.astype(f32) / inner_gain.astype(f32)
    gated_squares = jnp.sum(ungained * ungained, axis=1)
    high = gated_squares.astype(bf16)
    low = (gated_squares - high.astype(f32)).astype(bf16)
    out_part = product(all_low, w_out, bf16)
    shared = from_everyone(jnp.concatenate([out_part, high[None], low[None]], axis=0), "tp")
    shared = shared.astype(f32).sum(axis=0)
    out_sum, gated_total = shared[:batch], shared[batch] + shared[batch + 1]
    residual = (
        tokens.astype(f32) + out_sum * lax.rsqrt(gated_total / inner + epsilon)[:, None]
    ).astype(bf16)

    residual_wide = residual.astype(f32)
    hidden_low = (residual_wide * mlp_gain.astype(f32)).astype(bf16)
    row_squares = jnp.sum(residual_wide * residual_wide, axis=1, keepdims=True)
    up_part = jnp.concatenate([product(hidden_low, w_up, bf16), hi_lo(row_squares)], axis=1)
    up_mine = scattered_sum(scattered_sum(up_part, "near").astype(bf16), "far")
    up_share, square_share = up_mine[:, :-LANES], jnp.sum(up_mine[:, -LANES:], axis=1, keepdims=True)
    active = jnp.square(
        jax.nn.relu(up_share * lax.rsqrt(square_share / model + epsilon))
    ).astype(bf16)
    active = from_everyone(active, "far").reshape(-1, active.shape[1])
    active = from_everyone(active, "near").reshape(batch, -1)
    down_sum = from_everyone(product(active, w_down, bf16), "tp").astype(f32).sum(axis=0)
    return ((residual_wide + down_sum).astype(bf16), next_state)


def solution(mesh):
    kv = mesh.shape["kv"]
    near = NEAR if kv % NEAR == 0 else 1
    names = ("grp", "far", "near", "tp")
    split = Mesh(mesh.devices.reshape(mesh.shape["grp"], kv // near, near, mesh.shape["tp"]), names)
    kv = ("far", "near")
    seq = ("grp", "far", "near")
    return jax.shard_map(
        per_device,
        mesh=split,
        in_specs=(
            P("grp", kv),
            P(seq),
            P(seq, None, "tp"),
            P(seq, None, None, "tp"),
            P(seq, "tp", None, None),
            P(kv),
            P(kv, "tp"),
            P(kv, "tp"),
            P(kv, "tp"),
            P(kv, "tp"),
            P(kv, "tp"),
            P("tp"),
            P("tp"),
            P(None, "tp"),
            P(None, None, "tp"),
            P("tp"),
            P("tp", kv),
            P(kv),
            P(kv, "tp"),
            P("tp", kv),
        ),
        out_specs=(P("grp", kv), P(seq, "tp", None, None)),
        check_vma=False,
    )
```

```python
import functools

import jax
import jax.numpy as jnp
from jax import lax
from jax.experimental import pallas as pl
from jax.sharding import Mesh, PartitionSpec as P

HEAD_DIM = 64
STATE = 128
CONV_WIDTH = 4
LANES = 128
NEAR = 4

epsilon = 1e-06
f32, bf16 = jnp.float32, jnp.bfloat16


def scattered_sum(rows, along):
    size = lax.axis_size(along)
    parts = rows.reshape(size, -1, rows.shape[1])
    return lax.all_to_all(parts, along, 0, 0, tiled=True).astype(f32).sum(axis=0)


def from_everyone(shard, along):
    copies = jnp.broadcast_to(shard, (lax.axis_size(along), *shard.shape))
    return lax.all_to_all(copies, along, 0, 0, tiled=True)


def hi_lo(column):
    hi = column.astype(bf16)
    lo = (column - hi.astype(f32)).astype(bf16)
    lane = lax.broadcasted_iota(jnp.int32, (column.shape[0], LANES), 1)
    return jnp.where(lane == 0, hi, jnp.where(lane == 1, lo, jnp.zeros((), bf16)))


def project_kernel(
    far, near, seqs, tokens_ref, gain_ref, gate_ref, value_ref, key_ref, query_ref, step_ref, sent_ref
):
    batch, width = tokens_ref.shape
    to = lax.broadcasted_iota(jnp.int32, (batch, batch), 0)
    at = lax.broadcasted_iota(jnp.int32, (batch, batch), 1)
    group = to // (far * seqs)
    rest = to - group * (far * seqs)
    block = rest // seqs
    source = (block * near + group) * seqs + rest - block * seqs
    order = jnp.where(at == source, 1.0, 0.0).astype(bf16)
    wide = product(order, tokens_ref[...])
    scaled = (wide * gain_ref[...].astype(f32)).astype(bf16)
    column = 0
    for weight in (gate_ref, value_ref, key_ref, query_ref):
        size = weight.shape[1]
        sent_ref[:, column : column + size] = product(scaled, weight[...]).astype(bf16)
        column += size
    heads = step_ref.shape[0]
    steps = jnp.concatenate(
        [step_ref[...].astype(f32), jnp.zeros((LANES - heads, width), f32)], axis=0
    ).astype(bf16)
    steps = lax.dot_general(
        scaled, steps, (((1,), (1,)), ((), ())), preferred_element_type=f32
    )
    squares = jnp.sum(wide * wide, axis=1, keepdims=True)
    high = squares.astype(bf16).astype(f32)
    lane = lax.broadcasted_iota(jnp.int32, (batch, LANES), 1)
    steps = jnp.where(lane == heads, high, jnp.where(lane == heads + 1, squares - high, steps))
    sent_ref[:, column : column + LANES] = steps.astype(bf16)
    sent_ref[:, column + LANES :] = wide.astype(bf16)


def project(tokens, norm_gain, w_gate, w_value, w_key, w_query, w_step, far, near):
    batch, width = tokens.shape
    columns = sum(w.shape[1] for w in (w_gate, w_value, w_key, w_query)) + LANES + width
    return pl.pallas_call(
        functools.partial(project_kernel, far, near, batch // (far * near)),
        out_shape=jax.ShapeDtypeStruct((batch, columns), bf16),
        cost_estimate=pl.CostEstimate(
            flops=2 * batch * width * columns,
            bytes_accessed=2 * columns * (batch + width),
            transcendentals=0,
        ),
        name="project",
    )(tokens, norm_gain[None], w_gate, w_value, w_key, w_query, w_step.T)


def causal_conv(state_rows, newest, conv_weights):
    extended = jnp.concatenate([state_rows, newest[:, None]], axis=1)
    conv_sum = extended[:, 0] * conv_weights[0].astype(f32)
    for offset in range(1, conv_weights.shape[0]):
        conv_sum = conv_sum + extended[:, offset] * conv_weights[offset].astype(f32)
    return jax.nn.silu(conv_sum)


def product(left, right, out=f32):
    return jnp.dot(left, right, preferred_element_type=out)


def per_device(
    tokens,
    lengths,
    conv_state_x,
    conv_state_bc,
    ssm_state,
    norm_gain,
    w_gate,
    w_value,
    w_key,
    w_query,
    w_step,
    step_bias,
    decay_log,
    conv_x,
    conv_bc,
    inner_gain,
    w_out,
    mlp_gain,
    w_up,
    w_down,
):
    far, near = lax.axis_size("far"), lax.axis_size("near")
    head_count = w_step.shape[1]
    group_count = w_key.shape[1] // STATE
    per_group = head_count // group_count
    batch, width = tokens.shape
    model = width * far * near
    inner = w_gate.shape[1] * lax.axis_size("tp")
    seqs = batch // (far * near)

    sent = project(tokens, norm_gain, w_gate, w_value, w_key, w_query, w_step, far, near)
    cols = sent.shape[1] - width
    came = lax.all_to_all(sent.reshape(near, -1, cols + width), "near", 0, 0, tiled=True)
    near_sum = came[:, :, :cols].astype(f32).sum(axis=0).astype(bf16)
    near_tokens = came[:, :, cols:].swapaxes(0, 1).reshape(-1, near * width)
    mine = scattered_sum(near_sum, "far")

    hidden = w_up.shape[1] // near
    blocks = hidden // width
    extra = jnp.concatenate(
        [jnp.broadcast_to(mlp_gain[None], (8, width)), near_sum[:8, :width]], axis=0
    )
    packed = jnp.concatenate(
        [
            w_up.reshape(width, near, blocks, width).transpose(1, 2, 0, 3).reshape(near, -1, width),
            w_down.reshape(near, -1, width),
            jnp.broadcast_to(w_out[None], (near, *w_out.shape)),
            jnp.broadcast_to(extra[None], (near, *extra.shape)),
        ],
        axis=1,
    )
    here = lax.axis_index("near")
    pieces = []
    for step in range(near):
        piece = lax.dynamic_index_in_dim(packed, here ^ step, keepdims=False)
        if step:
            with jax.named_scope("swap"):
                piece = lax.ppermute(piece, "near", [(i, i ^ step) for i in range(near)])
        pieces.append(piece)
    pieces = jnp.stack(pieces)
    swapped = jnp.stack(
        [lax.dynamic_index_in_dim(pieces, here ^ i, keepdims=False) for i in range(near)]
    )
    own_up = swapped[:, :hidden].reshape(near, blocks, width, width)
    own_up = own_up.transpose(0, 2, 1, 3).reshape(near * width, hidden)
    own_down = swapped[:, hidden : 2 * hidden]
    own_out = swapped[:, 2 * hidden : 2 * hidden + w_out.shape[0]]
    near_gain = swapped[:, 2 * hidden + w_out.shape[0]].reshape(1, near * width)

    cuts, at = [], 0
    for size in (w_gate.shape[1], w_value.shape[1], w_key.shape[1], w_query.shape[1], head_count):
        cuts.append(mine[:, at : at + size])
        at += size
    gate_raw, value_raw, key_raw, query_raw, step_raw = cuts
    squares = jnp.sum(mine[:, at:], axis=1, keepdims=True)
    inverse = lax.rsqrt(squares / model + epsilon)

    row_live = (
        jnp.arange(CONV_WIDTH - 1, dtype=jnp.int32)[None, :] >= CONV_WIDTH - 1 - lengths[:, None]
    ).astype(f32)
    live_x = conv_state_x.astype(f32) * row_live[:, :, None]
    live_bc = conv_state_bc.astype(f32) * row_live[:, :, None, None]
    mixed_values = causal_conv(live_x, value_raw * inverse, conv_x).reshape(
        seqs, head_count, HEAD_DIM
    )
    key_query = causal_conv(
        live_bc, jnp.stack([key_raw * inverse, query_raw * inverse], axis=1), conv_bc
    )
    key_heads = jnp.repeat(key_query[:, 0].reshape(seqs, group_count, STATE), per_group, axis=1)
    query_heads = jnp.repeat(key_query[:, 1].reshape(seqs, group_count, STATE), per_group, axis=1)
    step_size = jax.nn.softplus(step_raw * inverse + step_bias)
    rate_now = -jnp.exp(decay_log) * step_size
    next_state = (
        ssm_state * jnp.exp(rate_now)[:, :, None, None]
        + (step_size[:, :, None] * mixed_values)[:, :, :, None] * key_heads[:, :, None, :]
    )
    mixer_y = jnp.sum(next_state * query_heads[:, :, None, :], axis=3).reshape(
        seqs, head_count * HEAD_DIM
    )
    gated_rows = mixer_y * jax.nn.silu(gate_raw * inverse)
    gated_low = (gated_rows * inner_gain.astype(f32)).astype(bf16)

    all_low = from_everyone(gated_low, "far").reshape(far * seqs, -1)
    ungained = all_low.astype(f32) / inner_gain.astype(f32)
    gated_squares = hi_lo(jnp.sum(ungained * ungained, axis=1, keepdims=True))
    out_part = [product(all_low, own_out[i], bf16) for i in range(near)]
    shared = from_everyone(jnp.concatenate([*out_part, gated_squares], axis=1), "tp")
    shared = shared.astype(f32).sum(axis=0)
    gated_total = jnp.sum(shared[:, near * width :], axis=1, keepdims=True)
    residual = (
        near_tokens.astype(f32)
        + shared[:, : near * width] * lax.rsqrt(gated_total / inner + epsilon)
    ).astype(bf16)

    residual = from_everyone(residual, "near").reshape(batch, near * width)
    residual_wide = residual.astype(f32)
    hidden_low = (residual_wide * near_gain.astype(f32)).astype(bf16)
    row_squares = jnp.sum(residual_wide * residual_wide, axis=1, keepdims=True)
    up_part = jnp.concatenate([product(hidden_low, own_up, bf16), hi_lo(row_squares)], axis=1)
    up_mine = scattered_sum(up_part, "far")
    up_share, square_share = up_mine[:, :hidden], jnp.sum(up_mine[:, hidden:], axis=1, keepdims=True)
    active = jnp.square(
        jax.nn.relu(up_share * lax.rsqrt(square_share / model + epsilon))
    ).astype(bf16)
    active = from_everyone(active, "far").reshape(batch, hidden)
    tp = lax.axis_size("tp")
    down_part = jnp.stack([product(active, own_down[i], bf16) for i in range(near)])
    down_part = down_part.reshape(near * tp, batch // tp, width)
    down_sum = lax.all_to_all(down_part, ("near", "tp"), 0, 0, tiled=True).astype(f32).sum(axis=0)
    own_rows = residual.reshape(tp, batch // tp, near, width).swapaxes(1, 2)
    own_rows = own_rows[lax.axis_index("tp"), lax.axis_index("near")]
    finished = (own_rows.astype(f32) + down_sum).astype(bf16)
    finished = from_everyone(finished, "tp").reshape(near, far, seqs, width)
    return (finished.swapaxes(0, 1).reshape(batch, width), next_state)


def solution(mesh):
    kv = mesh.shape["kv"]
    near = NEAR if kv % NEAR == 0 else 1
    names = ("grp", "far", "near", "tp")
    split = Mesh(mesh.devices.reshape(mesh.shape["grp"], kv // near, near, mesh.shape["tp"]), names)
    kv = ("far", "near")
    seq = ("grp", "far", "near")
    return jax.shard_map(
        per_device,
        mesh=split,
        in_specs=(
            P("grp", kv),
            P(seq),
            P(seq, None, "tp"),
            P(seq, None, None, "tp"),
            P(seq, "tp", None, None),
            P(kv),
            P(kv, "tp"),
            P(kv, "tp"),
            P(kv, "tp"),
            P(kv, "tp"),
            P(kv, "tp"),
            P("tp"),
            P("tp"),
            P(None, "tp"),
            P(None, None, "tp"),
            P("tp"),
            P("tp", kv),
            P(kv),
            P(kv, "tp"),
            P("tp", kv),
        ),
        out_specs=(P("grp", kv), P(seq, "tp", None, None)),
        check_vma=False,
    )
```

```python
import functools

import jax
import jax.numpy as jnp
from jax import lax
from jax.experimental import pallas as pl
from jax.sharding import Mesh, PartitionSpec as P


HEAD_DIM = 64
STATE = 128
CONV_WIDTH = 4
LANES = 128
NEAR = 4

epsilon = 1e-06
f32, bf16 = jnp.float32, jnp.bfloat16


def scattered_sum(rows, along):
    size = lax.axis_size(along)
    parts = rows.reshape(size, -1, rows.shape[1])
    return lax.all_to_all(parts, along, 0, 0, tiled=True).astype(f32).sum(axis=0)


def from_everyone(shard, along):
    copies = jnp.broadcast_to(shard, (lax.axis_size(along), *shard.shape))
    return lax.all_to_all(copies, along, 0, 0, tiled=True)


def hi_lo(column):
    hi = column.astype(bf16)
    lo = (column - hi.astype(f32)).astype(bf16)
    lane = lax.broadcasted_iota(jnp.int32, (column.shape[0], LANES), 1)
    return jnp.where(lane == 0, hi, jnp.where(lane == 1, lo, jnp.zeros((), bf16)))


def project_kernel(
    far, near, seqs, tokens_ref, gain_ref, gate_ref, value_ref, key_ref, query_ref, step_ref, sent_ref
):
    batch, width = tokens_ref.shape
    to = lax.broadcasted_iota(jnp.int32, (batch, batch), 0)
    at = lax.broadcasted_iota(jnp.int32, (batch, batch), 1)
    group = to // (far * seqs)
    rest = to - group * (far * seqs)
    block = rest // seqs
    source = (block * near + group) * seqs + rest - block * seqs
    order = jnp.where(at == source, 1.0, 0.0).astype(bf16)
    wide = product(order, tokens_ref[...])
    scaled = (wide * gain_ref[...].astype(f32)).astype(bf16)
    column = 0
    for weight in (gate_ref, value_ref, key_ref, query_ref):
        size = weight.shape[1]
        sent_ref[:, column : column + size] = product(scaled, weight[...]).astype(bf16)
        column += size
    heads = step_ref.shape[0]
    steps = jnp.concatenate(
        [step_ref[...].astype(f32), jnp.zeros((LANES - heads, width), f32)], axis=0
    ).astype(bf16)
    steps = lax.dot_general(
        scaled, steps, (((1,), (1,)), ((), ())), preferred_element_type=f32
    )
    squares = jnp.sum(wide * wide, axis=1, keepdims=True)
    high = squares.astype(bf16).astype(f32)
    lane = lax.broadcasted_iota(jnp.int32, (batch, LANES), 1)
    steps = jnp.where(lane == heads, high, jnp.where(lane == heads + 1, squares - high, steps))
    sent_ref[:, column : column + LANES] = steps.astype(bf16)
    sent_ref[:, column + LANES :] = wide.astype(bf16)


def project(tokens, norm_gain, w_gate, w_value, w_key, w_query, w_step, far, near):
    batch, width = tokens.shape
    columns = sum(w.shape[1] for w in (w_gate, w_value, w_key, w_query)) + LANES + width
    return pl.pallas_call(
        functools.partial(project_kernel, far, near, batch // (far * near)),
        out_shape=jax.ShapeDtypeStruct((batch, columns), bf16),
        cost_estimate=pl.CostEstimate(
            flops=2 * batch * width * columns,
            bytes_accessed=2 * columns * (batch + width),
            transcendentals=0,
        ),
        name="project",
    )(tokens, norm_gain[None], w_gate, w_value, w_key, w_query, w_step.T)


def causal_conv(state_rows, newest, conv_weights):
    extended = jnp.concatenate([state_rows, newest[:, None]], axis=1)
    conv_sum = extended[:, 0] * conv_weights[0].astype(f32)
    for offset in range(1, conv_weights.shape[0]):
        conv_sum = conv_sum + extended[:, offset] * conv_weights[offset].astype(f32)
    return jax.nn.silu(conv_sum)


def product(left, right, out=f32):
    return jnp.dot(left, right, preferred_element_type=out)


def per_device(
    tokens,
    lengths,
    conv_state_x,
    conv_state_bc,
    ssm_state,
    norm_gain,
    w_gate,
    w_value,
    w_key,
    w_query,
    w_step,
    step_bias,
    decay_log,
    conv_x,
    conv_bc,
    inner_gain,
    w_out,
    mlp_gain,
    w_up,
    w_down,
):
    far, near = lax.axis_size("far"), lax.axis_size("near")
    head_count = w_step.shape[1]
    group_count = w_key.shape[1] // STATE
    per_group = head_count // group_count
    batch, width = tokens.shape
    model = width * far * near
    inner = w_gate.shape[1] * lax.axis_size("tp")
    seqs = batch // (far * near)

    sent = project(tokens, norm_gain, w_gate, w_value, w_key, w_query, w_step, far, near)
    cols = sent.shape[1] - width
    came = lax.all_to_all(sent.reshape(near, -1, cols + width), "near", 0, 0, tiled=True)
    near_sum = came[:, :, :cols].astype(f32).sum(axis=0).astype(bf16)
    near_tokens = came[:, :, cols:].swapaxes(0, 1).reshape(-1, near * width)
    mine = scattered_sum(near_sum, "far")

    hidden = w_up.shape[1] // near
    blocks = hidden // width
    extra = jnp.concatenate(
        [jnp.broadcast_to(mlp_gain[None], (8, width)), near_sum[:8, :width]], axis=0
    )
    packed = jnp.concatenate(
        [
            w_up.reshape(width, near, blocks, width).transpose(1, 2, 0, 3).reshape(near, -1, width),
            w_down.reshape(near, -1, width),
            jnp.broadcast_to(w_out[None], (near, *w_out.shape)),
            jnp.broadcast_to(extra[None], (near, *extra.shape)),
        ],
        axis=1,
    )
    here = lax.axis_index("near")
    pieces = []
    for step in range(near):
        piece = lax.dynamic_index_in_dim(packed, here ^ step, keepdims=False)
        if step:
            piece = lax.ppermute(piece, "near", [(i, i ^ step) for i in range(near)])
        pieces.append(piece)
    pieces = jnp.stack(pieces)
    swapped = jnp.stack(
        [lax.dynamic_index_in_dim(pieces, here ^ i, keepdims=False) for i in range(near)]
    )
    own_up = swapped[:, :hidden].reshape(near, blocks, width, width)
    own_up = own_up.transpose(0, 2, 1, 3).reshape(near * width, hidden)
    own_down = swapped[:, hidden : 2 * hidden]
    own_out = swapped[:, 2 * hidden : 2 * hidden + w_out.shape[0]]
    near_gain = swapped[:, 2 * hidden + w_out.shape[0]].reshape(1, near * width).astype(f32)
    rows = near_tokens.reshape(lax.axis_size("tp"), -1, near * width)
    own_tokens = rows[lax.axis_index("tp")]
    own_up, own_down, own_out, near_gain, own_tokens = lax.optimization_barrier(
        (own_up, own_down, own_out, near_gain, own_tokens)
    )

    cuts, at = [], 0
    for size in (w_gate.shape[1], w_value.shape[1], w_key.shape[1], w_query.shape[1], head_count):
        cuts.append(mine[:, at : at + size])
        at += size
    gate_raw, value_raw, key_raw, query_raw, step_raw = cuts
    squares = jnp.sum(mine[:, at:], axis=1, keepdims=True)
    inverse = lax.rsqrt(squares / model + epsilon)

    row_live = (
        jnp.arange(CONV_WIDTH - 1, dtype=jnp.int32)[None, :] >= CONV_WIDTH - 1 - lengths[:, None]
    ).astype(f32)
    live_x = conv_state_x.astype(f32) * row_live[:, :, None]
    live_bc = conv_state_bc.astype(f32) * row_live[:, :, None, None]
    mixed_values = causal_conv(live_x, value_raw * inverse, conv_x).reshape(
        seqs, head_count, HEAD_DIM
    )
    key_query = causal_conv(
        live_bc, jnp.stack([key_raw * inverse, query_raw * inverse], axis=1), conv_bc
    )
    key_heads = jnp.repeat(key_query[:, 0].reshape(seqs, group_count, STATE), per_group, axis=1)
    query_heads = jnp.repeat(key_query[:, 1].reshape(seqs, group_count, STATE), per_group, axis=1)
    step_size = jax.nn.softplus(step_raw * inverse + step_bias)
    rate_now = -jnp.exp(decay_log) * step_size
    next_state = (
        ssm_state * jnp.exp(rate_now)[:, :, None, None]
        + (step_size[:, :, None] * mixed_values)[:, :, :, None] * key_heads[:, :, None, :]
    )
    mixer_y = jnp.sum(next_state * query_heads[:, :, None, :], axis=3).reshape(
        seqs, head_count * HEAD_DIM
    )
    gated_rows = mixer_y * jax.nn.silu(gate_raw * inverse)
    gated_low = (gated_rows * inner_gain.astype(f32)).astype(bf16)

    all_low = from_everyone(gated_low, "far")
    all_low = all_low.reshape(far * seqs, -1)
    ungained = all_low.astype(f32) / inner_gain.astype(f32)
    gated_squares = hi_lo(jnp.sum(ungained * ungained, axis=1, keepdims=True))
    out_part = [product(all_low, own_out[i], bf16) for i in range(near)]
    tp = lax.axis_size("tp")
    shared = scattered_sum(jnp.concatenate([*out_part, gated_squares], axis=1), "tp")
    gated_total = jnp.sum(shared[:, near * width :], axis=1, keepdims=True)
    residual = (
        own_tokens.astype(f32)
        + shared[:, : near * width] * lax.rsqrt(gated_total / inner + epsilon)
    ).astype(bf16)

    residual = from_everyone(residual, ("near", "tp")).reshape(batch, near * width)
    residual_wide = residual.astype(f32)
    hidden_low = (residual_wide * near_gain).astype(bf16)
    row_squares = jnp.sum(residual_wide * residual_wide, axis=1, keepdims=True)
    up_part = jnp.concatenate([product(hidden_low, own_up, bf16), hi_lo(row_squares)], axis=1)
    own_rows = residual.reshape(tp, batch // tp, near, width).swapaxes(1, 2)
    own_rows = own_rows[lax.axis_index("tp"), lax.axis_index("near")]
    up_part, own_rows = lax.optimization_barrier((up_part, own_rows))
    up_mine = scattered_sum(up_part, "far")
    up_share, square_share = up_mine[:, :hidden], jnp.sum(up_mine[:, hidden:], axis=1, keepdims=True)
    active = jnp.square(
        jax.nn.relu(up_share * lax.rsqrt(square_share / model + epsilon))
    ).astype(bf16)
    active = from_everyone(active, "far").reshape(batch, hidden)
    down_part = jnp.stack([product(active, own_down[i], bf16) for i in range(near)])
    down_part = down_part.reshape(near * tp, batch // tp, width)
    down_sum = lax.all_to_all(down_part, ("near", "tp"), 0, 0, tiled=True).astype(f32).sum(axis=0)
    finished = (own_rows.astype(f32) + down_sum).astype(bf16)
    finished = from_everyone(finished, "tp").reshape(near, far, seqs, width)
    return (finished.swapaxes(0, 1).reshape(batch, width), next_state)


def solution(mesh):
    kv = mesh.shape["kv"]
    near = NEAR if kv % NEAR == 0 else 1
    names = ("grp", "far", "near", "tp")
    split = Mesh(mesh.devices.reshape(mesh.shape["grp"], kv // near, near, mesh.shape["tp"]), names)
    kv = ("far", "near")
    seq = ("grp", "far", "near")
    return jax.shard_map(
        per_device,
        mesh=split,
        in_specs=(
            P("grp", kv),
            P(seq),
            P(seq, None, "tp"),
            P(seq, None, None, "tp"),
            P(seq, "tp", None, None),
            P(kv),
            P(kv, "tp"),
            P(kv, "tp"),
            P(kv, "tp"),
            P(kv, "tp"),
            P(kv, "tp"),
            P("tp"),
            P("tp"),
            P(None, "tp"),
            P(None, None, "tp"),
            P("tp"),
            P("tp", kv),
            P(kv),
            P(kv, "tp"),
            P("tp", kv),
        ),
        out_specs=(P("grp", kv), P(seq, "tp", None, None)),
        check_vma=False,
    )
```

```python
import functools

import jax
import jax.numpy as jnp
from jax import lax
from jax.experimental import pallas as pl
from jax.sharding import Mesh, PartitionSpec as P


HEAD_DIM = 64
STATE = 128
CONV_WIDTH = 4
LANES = 128
NEAR = 4

epsilon = 1e-06
f32, bf16 = jnp.float32, jnp.bfloat16


def scattered_sum(rows, along):
    size = lax.axis_size(along)
    parts = rows.reshape(size, -1, rows.shape[1])
    return lax.all_to_all(parts, along, 0, 0, tiled=True).astype(f32).sum(axis=0)


def from_everyone(shard, along):
    copies = jnp.broadcast_to(shard, (lax.axis_size(along), *shard.shape))
    return lax.all_to_all(copies, along, 0, 0, tiled=True)


def hi_lo(column):
    hi = column.astype(bf16)
    lo = (column - hi.astype(f32)).astype(bf16)
    lane = lax.broadcasted_iota(jnp.int32, (column.shape[0], LANES), 1)
    return jnp.where(lane == 0, hi, jnp.where(lane == 1, lo, jnp.zeros((), bf16)))


def project_kernel(
    far, near, seqs, tokens_ref, gain_ref, gate_ref, value_ref, key_ref, query_ref, step_ref, sent_ref, rows_ref
):
    batch, width = tokens_ref.shape
    to = lax.broadcasted_iota(jnp.int32, (batch, batch), 0)
    at = lax.broadcasted_iota(jnp.int32, (batch, batch), 1)
    group = to // (far * seqs)
    rest = to - group * (far * seqs)
    block = rest // seqs
    source = (block * near + group) * seqs + rest - block * seqs
    order = jnp.where(at == source, 1.0, 0.0).astype(bf16)
    wide = product(order, tokens_ref[...])
    scaled = (wide * gain_ref[...].astype(f32)).astype(bf16)
    column = 0
    for weight in (gate_ref, value_ref, key_ref, query_ref):
        size = weight.shape[1]
        sent_ref[:, column : column + size] = product(scaled, weight[...]).astype(bf16)
        column += size
    heads = step_ref.shape[0]
    steps = jnp.concatenate(
        [step_ref[...].astype(f32), jnp.zeros((LANES - heads, width), f32)], axis=0
    ).astype(bf16)
    steps = lax.dot_general(
        scaled, steps, (((1,), (1,)), ((), ())), preferred_element_type=f32
    )
    squares = jnp.sum(wide * wide, axis=1, keepdims=True)
    high = squares.astype(bf16).astype(f32)
    lane = lax.broadcasted_iota(jnp.int32, (batch, LANES), 1)
    steps = jnp.where(lane == heads, high, jnp.where(lane == heads + 1, squares - high, steps))
    sent_ref[:, column:] = steps.astype(bf16)
    rows_ref[...] = wide.astype(bf16)


def project(tokens, norm_gain, w_gate, w_value, w_key, w_query, w_step, far, near):
    batch, width = tokens.shape
    columns = sum(w.shape[1] for w in (w_gate, w_value, w_key, w_query)) + LANES
    return pl.pallas_call(
        functools.partial(project_kernel, far, near, batch // (far * near)),
        out_shape=(
            jax.ShapeDtypeStruct((batch, columns), bf16),
            jax.ShapeDtypeStruct((batch, width), bf16),
        ),
        cost_estimate=pl.CostEstimate(
            flops=2 * batch * width * columns,
            bytes_accessed=2 * columns * (batch + width),
            transcendentals=0,
        ),
        name="project",
    )(tokens, norm_gain[None], w_gate, w_value, w_key, w_query, w_step.T)


def causal_conv(state_rows, newest, conv_weights):
    extended = jnp.concatenate([state_rows, newest[:, None]], axis=1)
    conv_sum = extended[:, 0] * conv_weights[0].astype(f32)
    for offset in range(1, conv_weights.shape[0]):
        conv_sum = conv_sum + extended[:, offset] * conv_weights[offset].astype(f32)
    return jax.nn.silu(conv_sum)


def product(left, right, out=f32):
    return jnp.dot(left, right, preferred_element_type=out)


def per_device(
    tokens,
    lengths,
    conv_state_x,
    conv_state_bc,
    ssm_state,
    norm_gain,
    w_gate,
    w_value,
    w_key,
    w_query,
    w_step,
    step_bias,
    decay_log,
    conv_x,
    conv_bc,
    inner_gain,
    w_out,
    mlp_gain,
    w_up,
    w_down,
):
    far, near = lax.axis_size("far"), lax.axis_size("near")
    head_count = w_step.shape[1]
    group_count = w_key.shape[1] // STATE
    per_group = head_count // group_count
    batch, width = tokens.shape
    model = width * far * near
    inner = w_gate.shape[1] * lax.axis_size("tp")
    seqs = batch // (far * near)

    sent, token_rows = project(
        tokens, norm_gain, w_gate, w_value, w_key, w_query, w_step, far, near
    )
    near_sum = scattered_sum(sent, "near").astype(bf16)
    mine = scattered_sum(near_sum, "far")

    hidden = w_up.shape[1] // near
    blocks = hidden // width
    extra = jnp.concatenate(
        [jnp.broadcast_to(mlp_gain[None], (8, width)), near_sum[:8, :width]], axis=0
    )
    packed = jnp.concatenate(
        [
            w_up.reshape(width, near, blocks, width).transpose(1, 2, 0, 3).reshape(near, -1, width),
            w_down.reshape(near, -1, width),
            jnp.broadcast_to(w_out[None], (near, *w_out.shape)),
            token_rows.reshape(near, -1, width),
            jnp.broadcast_to(extra[None], (near, *extra.shape)),
        ],
        axis=1,
    )
    here = lax.axis_index("near")
    pieces = []
    for step in range(near):
        piece = lax.dynamic_index_in_dim(packed, here ^ step, keepdims=False)
        if step:
            piece = lax.ppermute(piece, "near", [(i, i ^ step) for i in range(near)])
        pieces.append(piece)
    pieces = jnp.stack(pieces)
    swapped = jnp.stack(
        [lax.dynamic_index_in_dim(pieces, here ^ i, keepdims=False) for i in range(near)]
    )
    own_up = swapped[:, :hidden].reshape(near, blocks, width, width)
    own_up = own_up.transpose(0, 2, 1, 3).reshape(near * width, hidden)
    own_down = swapped[:, hidden : 2 * hidden]
    own_out = swapped[:, 2 * hidden : 2 * hidden + w_out.shape[0]]
    at = 2 * hidden + w_out.shape[0]
    near_tokens = swapped[:, at : at + batch // near].swapaxes(0, 1).reshape(-1, near * width)
    near_gain = swapped[:, at + batch // near].reshape(1, near * width).astype(f32)

    cuts, at = [], 0
    for size in (w_gate.shape[1], w_value.shape[1], w_key.shape[1], w_query.shape[1], head_count):
        cuts.append(mine[:, at : at + size])
        at += size
    gate_raw, value_raw, key_raw, query_raw, step_raw = cuts
    squares = jnp.sum(mine[:, at:], axis=1, keepdims=True)
    inverse = lax.rsqrt(squares / model + epsilon)

    row_live = (
        jnp.arange(CONV_WIDTH - 1, dtype=jnp.int32)[None, :] >= CONV_WIDTH - 1 - lengths[:, None]
    ).astype(f32)
    live_x = conv_state_x.astype(f32) * row_live[:, :, None]
    live_bc = conv_state_bc.astype(f32) * row_live[:, :, None, None]
    mixed_values = causal_conv(live_x, value_raw * inverse, conv_x).reshape(
        seqs, head_count, HEAD_DIM
    )
    key_query = causal_conv(
        live_bc, jnp.stack([key_raw * inverse, query_raw * inverse], axis=1), conv_bc
    )
    key_heads = jnp.repeat(key_query[:, 0].reshape(seqs, group_count, STATE), per_group, axis=1)
    query_heads = jnp.repeat(key_query[:, 1].reshape(seqs, group_count, STATE), per_group, axis=1)
    step_size = jax.nn.softplus(step_raw * inverse + step_bias)
    decay = jnp.exp(-jnp.exp(decay_log) * step_size)
    fed = step_size[:, :, None] * mixed_values
    overlap = jnp.sum(key_heads * query_heads, axis=2)
    mixer_y = (
        decay[:, :, None] * jnp.sum(ssm_state * query_heads[:, :, None, :], axis=3)
        + fed * overlap[:, :, None]
    ).reshape(seqs, head_count * HEAD_DIM)
    gated_rows = mixer_y * jax.nn.silu(gate_raw * inverse)
    gated_low = (gated_rows * inner_gain.astype(f32)).astype(bf16)
    gated_low, old_state = lax.optimization_barrier((gated_low, ssm_state))
    next_state = old_state * decay[:, :, None, None] + fed[:, :, :, None] * key_heads[:, :, None, :]
    picks = [here == i for i in range(near)]
    own_up, own_down, own_out, near_gain, near_tokens, next_state, picks = lax.optimization_barrier(
        (own_up, own_down, own_out, near_gain, near_tokens, next_state, picks)
    )

    all_low = from_everyone(gated_low, "far")
    all_low = all_low.reshape(far * seqs, -1)
    ungained = all_low.astype(f32) / inner_gain.astype(f32)
    gated_squares = hi_lo(jnp.sum(ungained * ungained, axis=1, keepdims=True))
    out_part = [product(all_low, own_out[i], bf16) for i in range(near)]
    shared = from_everyone(jnp.concatenate([*out_part, gated_squares], axis=1), "tp")
    shared = shared.astype(f32).sum(axis=0)
    gated_total = jnp.sum(shared[:, near * width :], axis=1, keepdims=True)
    residual = (
        near_tokens.astype(f32)
        + shared[:, : near * width] * lax.rsqrt(gated_total / inner + epsilon)
    ).astype(bf16)

    residual = from_everyone(residual, "near").reshape(batch, near * width)
    residual_wide = residual.astype(f32)
    hidden_low = (residual_wide * near_gain).astype(bf16)
    row_squares = jnp.sum(residual_wide * residual_wide, axis=1, keepdims=True)
    up_part = jnp.concatenate([product(hidden_low, own_up, bf16), hi_lo(row_squares)], axis=1)
    own_rows = residual[:, :width]
    for i in range(1, near):
        own_rows = jnp.where(picks[i], residual[:, i * width : (i + 1) * width], own_rows)
    up_part, own_rows = lax.optimization_barrier((up_part, own_rows))
    up_mine = scattered_sum(up_part, "far")
    up_share, square_share = up_mine[:, :hidden], jnp.sum(up_mine[:, hidden:], axis=1, keepdims=True)
    active = jnp.square(
        jax.nn.relu(up_share * lax.rsqrt(square_share / model + epsilon))
    ).astype(bf16)
    active = from_everyone(active, "far").reshape(batch, hidden)
    down_part = jnp.stack([product(active, own_down[i], bf16) for i in range(near)])
    down_sum = lax.all_to_all(down_part, "near", 0, 0, tiled=True).astype(f32).sum(axis=0)
    down_sum = from_everyone(down_sum.astype(bf16), "tp").astype(f32).sum(axis=0)
    finished = (own_rows.astype(f32) + down_sum).astype(bf16).reshape(near, far, seqs, width)
    return (finished.swapaxes(0, 1).reshape(batch, width), next_state)


def solution(mesh):
    kv = mesh.shape["kv"]
    near = NEAR if kv % NEAR == 0 else 1
    names = ("grp", "far", "near", "tp")
    split = Mesh(mesh.devices.reshape(mesh.shape["grp"], kv // near, near, mesh.shape["tp"]), names)
    kv = ("far", "near")
    seq = ("grp", "far", "near")
    return jax.shard_map(
        per_device,
        mesh=split,
        in_specs=(
            P("grp", kv),
            P(seq),
            P(seq, None, "tp"),
            P(seq, None, None, "tp"),
            P(seq, "tp", None, None),
            P(kv),
            P(kv, "tp"),
            P(kv, "tp"),
            P(kv, "tp"),
            P(kv, "tp"),
            P(kv, "tp"),
            P("tp"),
            P("tp"),
            P(None, "tp"),
            P(None, None, "tp"),
            P("tp"),
            P("tp", kv),
            P(kv),
            P(kv, "tp"),
            P("tp", kv),
        ),
        out_specs=(P("grp", kv), P(seq, "tp", None, None)),
        check_vma=False,
    )
```

```python
import functools

import jax
import jax.numpy as jnp
from jax import lax
from jax.experimental import pallas as pl
from jax.sharding import Mesh, PartitionSpec as P


HEAD_DIM = 64
STATE = 128
CONV_WIDTH = 4
LANES = 128
NEAR = 4

epsilon = 1e-06
f32, bf16 = jnp.float32, jnp.bfloat16


def scattered_sum(rows, along):
    size = lax.axis_size(along)
    parts = rows.reshape(size, -1, rows.shape[1])
    return lax.all_to_all(parts, along, 0, 0, tiled=True).astype(f32).sum(axis=0)


def from_everyone(shard, along):
    copies = jnp.broadcast_to(shard, (lax.axis_size(along), *shard.shape))
    return lax.all_to_all(copies, along, 0, 0, tiled=True)


def in_turn(packed, here):
    near = packed.shape[0]
    pieces = []
    for step in range(near):
        piece = lax.dynamic_index_in_dim(packed, here ^ step, keepdims=False)
        if step:
            piece = lax.ppermute(piece, "near", [(i, i ^ step) for i in range(near)])
        pieces.append(piece)
    pieces = jnp.stack(pieces)
    return jnp.stack(
        [lax.dynamic_index_in_dim(pieces, here ^ i, keepdims=False) for i in range(near)]
    )


def hi_lo(column):
    hi = column.astype(bf16)
    lo = (column - hi.astype(f32)).astype(bf16)
    lane = lax.broadcasted_iota(jnp.int32, (column.shape[0], LANES), 1)
    return jnp.where(lane == 0, hi, jnp.where(lane == 1, lo, jnp.zeros((), bf16)))


def project_kernel(
    far, near, seqs, tokens_ref, gain_ref, gate_ref, value_ref, key_ref, query_ref, step_ref, sent_ref, rows_ref
):
    batch, width = tokens_ref.shape
    to = lax.broadcasted_iota(jnp.int32, (batch, batch), 0)
    at = lax.broadcasted_iota(jnp.int32, (batch, batch), 1)
    group = to // (far * seqs)
    rest = to - group * (far * seqs)
    block = rest // seqs
    source = (block * near + group) * seqs + rest - block * seqs
    order = jnp.where(at == source, 1.0, 0.0).astype(bf16)
    wide = product(order, tokens_ref[...])
    scaled = (wide * gain_ref[...].astype(f32)).astype(bf16)
    column = 0
    for weight in (gate_ref, value_ref, key_ref, query_ref):
        size = weight.shape[1]
        sent_ref[:, column : column + size] = product(scaled, weight[...]).astype(bf16)
        column += size
    heads = step_ref.shape[0]
    steps = jnp.concatenate(
        [step_ref[...].astype(f32), jnp.zeros((LANES - heads, width), f32)], axis=0
    ).astype(bf16)
    steps = lax.dot_general(
        scaled, steps, (((1,), (1,)), ((), ())), preferred_element_type=f32
    )
    squares = jnp.sum(wide * wide, axis=1, keepdims=True)
    high = squares.astype(bf16).astype(f32)
    lane = lax.broadcasted_iota(jnp.int32, (batch, LANES), 1)
    steps = jnp.where(lane == heads, high, jnp.where(lane == heads + 1, squares - high, steps))
    sent_ref[:, column:] = steps.astype(bf16)
    rows_ref[...] = wide.astype(bf16)


def project(tokens, norm_gain, w_gate, w_value, w_key, w_query, w_step, far, near):
    batch, width = tokens.shape
    columns = sum(w.shape[1] for w in (w_gate, w_value, w_key, w_query)) + LANES
    return pl.pallas_call(
        functools.partial(project_kernel, far, near, batch // (far * near)),
        out_shape=(
            jax.ShapeDtypeStruct((batch, columns), bf16),
            jax.ShapeDtypeStruct((batch, width), bf16),
        ),
        cost_estimate=pl.CostEstimate(
            flops=2 * batch * width * columns,
            bytes_accessed=2 * columns * (batch + width),
            transcendentals=0,
        ),
        name="project",
    )(tokens, norm_gain[None], w_gate, w_value, w_key, w_query, w_step.T)


def causal_conv(state_rows, newest, conv_weights):
    extended = jnp.concatenate([state_rows, newest[:, None]], axis=1)
    conv_sum = extended[:, 0] * conv_weights[0].astype(f32)
    for offset in range(1, conv_weights.shape[0]):
        conv_sum = conv_sum + extended[:, offset] * conv_weights[offset].astype(f32)
    return jax.nn.silu(conv_sum)


def product(left, right, out=f32):
    return jnp.dot(left, right, preferred_element_type=out)


def per_device(
    tokens,
    lengths,
    conv_state_x,
    conv_state_bc,
    ssm_state,
    norm_gain,
    w_gate,
    w_value,
    w_key,
    w_query,
    w_step,
    step_bias,
    decay_log,
    conv_x,
    conv_bc,
    inner_gain,
    w_out,
    mlp_gain,
    w_up,
    w_down,
):
    far, near = lax.axis_size("far"), lax.axis_size("near")
    head_count = w_step.shape[1]
    group_count = w_key.shape[1] // STATE
    per_group = head_count // group_count
    batch, width = tokens.shape
    model = width * far * near
    inner = w_gate.shape[1] * lax.axis_size("tp")
    seqs = batch // (far * near)

    sent, token_rows = project(
        tokens, norm_gain, w_gate, w_value, w_key, w_query, w_step, far, near
    )
    near_sum = scattered_sum(sent, "near").astype(bf16)
    mine = scattered_sum(near_sum, "far")

    hidden = w_up.shape[1] // near
    blocks = hidden // width
    extra = jnp.concatenate(
        [jnp.broadcast_to(mlp_gain[None], (8, width)), near_sum[:8, :width]], axis=0
    )
    packed = jnp.concatenate(
        [
            w_up.reshape(width, near, blocks, width).transpose(1, 2, 0, 3).reshape(near, -1, width),
            jnp.broadcast_to(w_out[None], (near, *w_out.shape)),
            token_rows.reshape(near, -1, width),
            jnp.broadcast_to(extra[None], (near, *extra.shape)),
        ],
        axis=1,
    )
    here = lax.axis_index("near")
    swapped = in_turn(packed, here)
    own_up = swapped[:, :hidden].reshape(near, blocks, width, width)
    own_up = own_up.transpose(0, 2, 1, 3).reshape(near * width, hidden)
    at = hidden + w_out.shape[0]
    own_out = swapped[:, hidden:at]
    near_tokens = swapped[:, at : at + batch // near].swapaxes(0, 1).reshape(-1, near * width)
    near_gain = swapped[:, at + batch // near].reshape(1, near * width).astype(f32)

    cuts, at = [], 0
    for size in (w_gate.shape[1], w_value.shape[1], w_key.shape[1], w_query.shape[1], head_count):
        cuts.append(mine[:, at : at + size])
        at += size
    gate_raw, value_raw, key_raw, query_raw, step_raw = cuts
    squares = jnp.sum(mine[:, at:], axis=1, keepdims=True)
    inverse = lax.rsqrt(squares / model + epsilon)

    row_live = (
        jnp.arange(CONV_WIDTH - 1, dtype=jnp.int32)[None, :] >= CONV_WIDTH - 1 - lengths[:, None]
    ).astype(f32)
    live_x = conv_state_x.astype(f32) * row_live[:, :, None]
    live_bc = conv_state_bc.astype(f32) * row_live[:, :, None, None]
    mixed_values = causal_conv(live_x, value_raw * inverse, conv_x).reshape(
        seqs, head_count, HEAD_DIM
    )
    key_query = causal_conv(
        live_bc, jnp.stack([key_raw * inverse, query_raw * inverse], axis=1), conv_bc
    )
    key_heads = jnp.repeat(key_query[:, 0].reshape(seqs, group_count, STATE), per_group, axis=1)
    query_heads = jnp.repeat(key_query[:, 1].reshape(seqs, group_count, STATE), per_group, axis=1)
    step_size = jax.nn.softplus(step_raw * inverse + step_bias)
    decay = jnp.exp(-jnp.exp(decay_log) * step_size)
    fed = step_size[:, :, None] * mixed_values
    overlap = jnp.sum(key_heads * query_heads, axis=2)
    mixer_y = (
        decay[:, :, None] * jnp.sum(ssm_state * query_heads[:, :, None, :], axis=3)
        + fed * overlap[:, :, None]
    ).reshape(seqs, head_count * HEAD_DIM)
    gated_rows = mixer_y * jax.nn.silu(gate_raw * inverse)
    gated_low = (gated_rows * inner_gain.astype(f32)).astype(bf16)
    gated_low, old_state = lax.optimization_barrier((gated_low, ssm_state))
    next_state = old_state * decay[:, :, None, None] + fed[:, :, :, None] * key_heads[:, :, None, :]
    picks = [here == i for i in range(near)]
    own_up, own_out, near_gain, near_tokens, next_state, picks = lax.optimization_barrier(
        (own_up, own_out, near_gain, near_tokens, next_state, picks)
    )

    all_low = from_everyone(gated_low, "far")
    all_low = all_low.reshape(far * seqs, -1)
    ungained = all_low.astype(f32) / inner_gain.astype(f32)
    gated_squares = hi_lo(jnp.sum(ungained * ungained, axis=1, keepdims=True))
    out_part = [product(all_low, own_out[i], bf16) for i in range(near)]
    shared = from_everyone(jnp.concatenate([*out_part, gated_squares], axis=1), "tp")
    shared = shared.astype(f32).sum(axis=0)
    gated_total = jnp.sum(shared[:, near * width :], axis=1, keepdims=True)
    residual = (
        near_tokens.astype(f32)
        + shared[:, : near * width] * lax.rsqrt(gated_total / inner + epsilon)
    ).astype(bf16)

    residual = from_everyone(residual, "near")
    residual = residual.reshape(batch, near * width)
    residual_wide = residual.astype(f32)
    hidden_low = (residual_wide * near_gain).astype(bf16)
    row_squares = jnp.sum(residual_wide * residual_wide, axis=1, keepdims=True)
    up_part = jnp.concatenate([product(hidden_low, own_up, bf16), hi_lo(row_squares)], axis=1)
    own_rows = residual[:, :width]
    for i in range(1, near):
        own_rows = jnp.where(picks[i], residual[:, i * width : (i + 1) * width], own_rows)
    up_part, own_rows = lax.optimization_barrier((up_part, own_rows))
    up_mine = scattered_sum(up_part, "far")
    own_down = in_turn(w_down.reshape(near, hidden, width), here)
    up_share, square_share = up_mine[:, :hidden], jnp.sum(up_mine[:, hidden:], axis=1, keepdims=True)
    active = jnp.square(
        jax.nn.relu(up_share * lax.rsqrt(square_share / model + epsilon))
    ).astype(bf16)
    active = from_everyone(active, "far")
    active = active.reshape(batch, hidden)
    down_part = jnp.stack([product(active, own_down[i], bf16) for i in range(near)])
    down_sum = lax.all_to_all(down_part, "near", 0, 0, tiled=True).astype(f32).sum(axis=0)
    down_sum = from_everyone(down_sum.astype(bf16), "tp").astype(f32).sum(axis=0)
    finished = (own_rows.astype(f32) + down_sum).astype(bf16).reshape(near, far, seqs, width)
    return (finished.swapaxes(0, 1).reshape(batch, width), next_state)


def solution(mesh):
    kv = mesh.shape["kv"]
    near = NEAR if kv % NEAR == 0 else 1
    names = ("grp", "far", "near", "tp")
    split = Mesh(mesh.devices.reshape(mesh.shape["grp"], kv // near, near, mesh.shape["tp"]), names)
    kv = ("far", "near")
    seq = ("grp", "far", "near")
    return jax.shard_map(
        per_device,
        mesh=split,
        in_specs=(
            P("grp", kv),
            P(seq),
            P(seq, None, "tp"),
            P(seq, None, None, "tp"),
            P(seq, "tp", None, None),
            P(kv),
            P(kv, "tp"),
            P(kv, "tp"),
            P(kv, "tp"),
            P(kv, "tp"),
            P(kv, "tp"),
            P("tp"),
            P("tp"),
            P(None, "tp"),
            P(None, None, "tp"),
            P("tp"),
            P("tp", kv),
            P(kv),
            P(kv, "tp"),
            P("tp", kv),
        ),
        out_specs=(P("grp", kv), P(seq, "tp", None, None)),
        check_vma=False,
    )
```

```python
import functools

import jax
import jax.numpy as jnp
from jax import lax
from jax.experimental import pallas as pl
from jax.sharding import Mesh, PartitionSpec as P


HEAD_DIM = 64
STATE = 128
CONV_WIDTH = 4
LANES = 128
NEAR = 4

epsilon = 1e-06
f32, bf16 = jnp.float32, jnp.bfloat16


def scattered_sum(rows, along):
    size = lax.axis_size(along)
    parts = rows.reshape(size, -1, rows.shape[1])
    return lax.all_to_all(parts, along, 0, 0, tiled=True).astype(f32).sum(axis=0)


def from_everyone(shard, along):
    copies = jnp.broadcast_to(shard, (lax.axis_size(along), *shard.shape))
    return lax.all_to_all(copies, along, 0, 0, tiled=True)


def in_turn(packed, here):
    near = packed.shape[0]
    pieces = []
    for step in range(near):
        piece = lax.dynamic_index_in_dim(packed, here ^ step, keepdims=False)
        if step:
            piece = lax.ppermute(piece, "near", [(i, i ^ step) for i in range(near)])
        pieces.append(piece)
    pieces = jnp.stack(pieces)
    return jnp.stack(
        [lax.dynamic_index_in_dim(pieces, here ^ i, keepdims=False) for i in range(near)]
    )


def hi_lo(column):
    hi = column.astype(bf16)
    lo = (column - hi.astype(f32)).astype(bf16)
    lane = lax.broadcasted_iota(jnp.int32, (column.shape[0], LANES), 1)
    return jnp.where(lane == 0, hi, jnp.where(lane == 1, lo, jnp.zeros((), bf16)))


def project_kernel(
    far, near, seqs, tokens_ref, gain_ref, gate_ref, value_ref, key_ref, query_ref, step_ref, sent_ref, rows_ref
):
    batch, width = tokens_ref.shape
    to = lax.broadcasted_iota(jnp.int32, (batch, batch), 0)
    at = lax.broadcasted_iota(jnp.int32, (batch, batch), 1)
    group = to // (far * seqs)
    rest = to - group * (far * seqs)
    block = rest // seqs
    source = (block * near + group) * seqs + rest - block * seqs
    order = jnp.where(at == source, 1.0, 0.0).astype(bf16)
    wide = product(order, tokens_ref[...])
    scaled = (wide * gain_ref[...].astype(f32)).astype(bf16)
    column = 0
    for weight in (gate_ref, value_ref, key_ref, query_ref):
        size = weight.shape[1]
        sent_ref[:, column : column + size] = product(scaled, weight[...]).astype(bf16)
        column += size
    heads = step_ref.shape[0]
    steps = jnp.concatenate(
        [step_ref[...].astype(f32), jnp.zeros((LANES - heads, width), f32)], axis=0
    ).astype(bf16)
    steps = lax.dot_general(
        scaled, steps, (((1,), (1,)), ((), ())), preferred_element_type=f32
    )
    squares = jnp.sum(wide * wide, axis=1, keepdims=True)
    high = squares.astype(bf16).astype(f32)
    lane = lax.broadcasted_iota(jnp.int32, (batch, LANES), 1)
    steps = jnp.where(lane == heads, high, jnp.where(lane == heads + 1, squares - high, steps))
    sent_ref[:, column:] = steps.astype(bf16)
    rows_ref[...] = wide.astype(bf16)


def project(tokens, norm_gain, w_gate, w_value, w_key, w_query, w_step, far, near):
    batch, width = tokens.shape
    columns = sum(w.shape[1] for w in (w_gate, w_value, w_key, w_query)) + LANES
    return pl.pallas_call(
        functools.partial(project_kernel, far, near, batch // (far * near)),
        out_shape=(
            jax.ShapeDtypeStruct((batch, columns), bf16),
            jax.ShapeDtypeStruct((batch, width), bf16),
        ),
        cost_estimate=pl.CostEstimate(
            flops=2 * batch * width * columns,
            bytes_accessed=2 * columns * (batch + width),
            transcendentals=0,
        ),
        name="project",
    )(tokens, norm_gain[None], w_gate, w_value, w_key, w_query, w_step.T)


def causal_conv(state_rows, newest, conv_weights):
    extended = jnp.concatenate([state_rows, newest[:, None]], axis=1)
    conv_sum = extended[:, 0] * conv_weights[0].astype(f32)
    for offset in range(1, conv_weights.shape[0]):
        conv_sum = conv_sum + extended[:, offset] * conv_weights[offset].astype(f32)
    return jax.nn.silu(conv_sum)


def product(left, right, out=f32):
    return jnp.dot(left, right, preferred_element_type=out)


def per_device(
    tokens,
    lengths,
    conv_state_x,
    conv_state_bc,
    ssm_state,
    norm_gain,
    w_gate,
    w_value,
    w_key,
    w_query,
    w_step,
    step_bias,
    decay_log,
    conv_x,
    conv_bc,
    inner_gain,
    w_out,
    mlp_gain,
    w_up,
    w_down,
):
    far, near = lax.axis_size("far"), lax.axis_size("near")
    head_count = w_step.shape[1]
    group_count = w_key.shape[1] // STATE
    per_group = head_count // group_count
    batch, width = tokens.shape
    model = width * far * near
    inner = w_gate.shape[1] * lax.axis_size("tp")
    seqs = batch // (far * near)

    sent, token_rows = project(
        tokens, norm_gain, w_gate, w_value, w_key, w_query, w_step, far, near
    )
    near_sum = scattered_sum(sent, "near").astype(bf16)
    mine = scattered_sum(near_sum, "far")

    hidden = w_up.shape[1] // near
    blocks = hidden // width
    extra = jnp.concatenate(
        [jnp.broadcast_to(mlp_gain[None], (8, width)), near_sum[:8, :width]], axis=0
    )
    packed = jnp.concatenate(
        [
            w_up.reshape(width, near, blocks, width).transpose(1, 2, 0, 3).reshape(near, -1, width),
            jnp.broadcast_to(w_out[None], (near, *w_out.shape)),
            token_rows.reshape(near, -1, width),
            jnp.broadcast_to(extra[None], (near, *extra.shape)),
        ],
        axis=1,
    )
    here = lax.axis_index("near")
    swapped = in_turn(packed, here)
    own_up = swapped[:, :hidden].reshape(near, blocks, width, width)
    own_up = own_up.transpose(0, 2, 1, 3).reshape(near * width, hidden)
    at = hidden + w_out.shape[0]
    own_out = swapped[:, hidden:at]
    near_tokens = swapped[:, at : at + batch // near].swapaxes(0, 1).reshape(-1, near * width)
    near_gain = swapped[:, at + batch // near].reshape(1, near * width).astype(f32)

    cuts, at = [], 0
    for size in (w_gate.shape[1], w_value.shape[1], w_key.shape[1], w_query.shape[1], head_count):
        cuts.append(mine[:, at : at + size])
        at += size
    gate_raw, value_raw, key_raw, query_raw, step_raw = cuts
    squares = jnp.sum(mine[:, at:], axis=1, keepdims=True)
    inverse = lax.rsqrt(squares / model + epsilon)

    row_live = (
        jnp.arange(CONV_WIDTH - 1, dtype=jnp.int32)[None, :] >= CONV_WIDTH - 1 - lengths[:, None]
    ).astype(f32)
    live_x = conv_state_x.astype(f32) * row_live[:, :, None]
    live_bc = conv_state_bc.astype(f32) * row_live[:, :, None, None]
    mixed_values = causal_conv(live_x, value_raw * inverse, conv_x).reshape(
        seqs, head_count, HEAD_DIM
    )
    key_query = causal_conv(
        live_bc, jnp.stack([key_raw * inverse, query_raw * inverse], axis=1), conv_bc
    )
    key_heads = jnp.repeat(key_query[:, 0].reshape(seqs, group_count, STATE), per_group, axis=1)
    query_heads = jnp.repeat(key_query[:, 1].reshape(seqs, group_count, STATE), per_group, axis=1)
    step_size = jax.nn.softplus(step_raw * inverse + step_bias)
    decay = jnp.exp(-jnp.exp(decay_log) * step_size)
    fed = step_size[:, :, None] * mixed_values
    overlap = jnp.sum(key_heads * query_heads, axis=2)
    mixer_y = (
        decay[:, :, None] * jnp.sum(ssm_state * query_heads[:, :, None, :], axis=3)
        + fed * overlap[:, :, None]
    ).reshape(seqs, head_count * HEAD_DIM)
    gated_rows = mixer_y * jax.nn.silu(gate_raw * inverse)
    gated_low = (gated_rows * inner_gain.astype(f32)).astype(bf16)
    gated_low, old_state = lax.optimization_barrier((gated_low, ssm_state))
    next_state = old_state * decay[:, :, None, None] + fed[:, :, :, None] * key_heads[:, :, None, :]
    own_tokens = near_tokens.reshape(lax.axis_size("tp"), -1, near * width)
    own_tokens = own_tokens[lax.axis_index("tp")]
    picks = [here == i for i in range(near)]
    own_up, own_out, near_gain, own_tokens, next_state, picks = lax.optimization_barrier(
        (own_up, own_out, near_gain, own_tokens, next_state, picks)
    )

    all_low = from_everyone(gated_low, "far")
    all_low = all_low.reshape(far * seqs, -1)
    ungained = all_low.astype(f32) / inner_gain.astype(f32)
    gated_squares = hi_lo(jnp.sum(ungained * ungained, axis=1, keepdims=True))
    out_part = [product(all_low, own_out[i], bf16) for i in range(near)]
    shared = scattered_sum(jnp.concatenate([*out_part, gated_squares], axis=1), "tp")
    gated_total = jnp.sum(shared[:, near * width :], axis=1, keepdims=True)
    residual = (
        own_tokens.astype(f32)
        + shared[:, : near * width] * lax.rsqrt(gated_total / inner + epsilon)
    ).astype(bf16)

    residual = from_everyone(residual, ("near", "tp"))
    residual = residual.reshape(batch, near * width)
    residual_wide = residual.astype(f32)
    hidden_low = (residual_wide * near_gain).astype(bf16)
    row_squares = jnp.sum(residual_wide * residual_wide, axis=1, keepdims=True)
    up_part = jnp.concatenate([product(hidden_low, own_up, bf16), hi_lo(row_squares)], axis=1)
    own_rows = residual[:, :width]
    for i in range(1, near):
        own_rows = jnp.where(picks[i], residual[:, i * width : (i + 1) * width], own_rows)
    up_part, own_rows = lax.optimization_barrier((up_part, own_rows))
    up_mine = scattered_sum(up_part, "far")
    own_down = in_turn(w_down.reshape(near, hidden, width), here)
    up_share, square_share = up_mine[:, :hidden], jnp.sum(up_mine[:, hidden:], axis=1, keepdims=True)
    active = jnp.square(
        jax.nn.relu(up_share * lax.rsqrt(square_share / model + epsilon))
    ).astype(bf16)
    active = from_everyone(active, "far")
    active = active.reshape(batch, hidden)
    down_part = jnp.stack([product(active, own_down[i], bf16) for i in range(near)])
    down_sum = lax.all_to_all(down_part, "near", 0, 0, tiled=True).astype(f32).sum(axis=0)
    down_sum = from_everyone(down_sum.astype(bf16), "tp").astype(f32).sum(axis=0)
    finished = (own_rows.astype(f32) + down_sum).astype(bf16).reshape(near, far, seqs, width)
    return (finished.swapaxes(0, 1).reshape(batch, width), next_state)


def solution(mesh):
    kv = mesh.shape["kv"]
    near = NEAR if kv % NEAR == 0 else 1
    names = ("grp", "far", "near", "tp")
    split = Mesh(mesh.devices.reshape(mesh.shape["grp"], kv // near, near, mesh.shape["tp"]), names)
    kv = ("far", "near")
    seq = ("grp", "far", "near")
    return jax.shard_map(
        per_device,
        mesh=split,
        in_specs=(
            P("grp", kv),
            P(seq),
            P(seq, None, "tp"),
            P(seq, None, None, "tp"),
            P(seq, "tp", None, None),
            P(kv),
            P(kv, "tp"),
            P(kv, "tp"),
            P(kv, "tp"),
            P(kv, "tp"),
            P(kv, "tp"),
            P("tp"),
            P("tp"),
            P(None, "tp"),
            P(None, None, "tp"),
            P("tp"),
            P("tp", kv),
            P(kv),
            P(kv, "tp"),
            P("tp", kv),
        ),
        out_specs=(P("grp", kv), P(seq, "tp", None, None)),
        check_vma=False,
    )
```

```python
import functools

import jax
import jax.numpy as jnp
from jax import lax
from jax.experimental import pallas as pl
from jax.sharding import Mesh, PartitionSpec as P


HEAD_DIM = 64
STATE = 128
CONV_WIDTH = 4
LANES = 128
NEAR = 4

epsilon = 1e-06
f32, bf16 = jnp.float32, jnp.bfloat16


def scattered_sum(rows, along):
    size = lax.axis_size(along)
    parts = rows.reshape(size, -1, rows.shape[1])
    return lax.all_to_all(parts, along, 0, 0, tiled=True).astype(f32).sum(axis=0)


def from_everyone(shard, along):
    copies = jnp.broadcast_to(shard, (lax.axis_size(along), *shard.shape))
    return lax.all_to_all(copies, along, 0, 0, tiled=True)


def in_turn(packed, here):
    near = packed.shape[0]
    pieces = []
    for step in range(near):
        piece = lax.dynamic_index_in_dim(packed, here ^ step, keepdims=False)
        if step:
            piece = lax.ppermute(piece, "near", [(i, i ^ step) for i in range(near)])
        pieces.append(piece)
    return pieces


def in_place(pieces, here):
    pieces = jnp.stack(pieces)
    return jnp.stack(
        [lax.dynamic_index_in_dim(pieces, here ^ i, keepdims=False) for i in range(len(pieces))]
    )


def hi_lo(column):
    hi = column.astype(bf16)
    lo = (column - hi.astype(f32)).astype(bf16)
    lane = lax.broadcasted_iota(jnp.int32, (column.shape[0], LANES), 1)
    return jnp.where(lane == 0, hi, jnp.where(lane == 1, lo, jnp.zeros((), bf16)))


def project_kernel(
    far, near, seqs, tokens_ref, gain_ref, gate_ref, value_ref, key_ref, query_ref, step_ref, sent_ref, rows_ref
):
    batch, width = tokens_ref.shape
    to = lax.broadcasted_iota(jnp.int32, (batch, batch), 0)
    at = lax.broadcasted_iota(jnp.int32, (batch, batch), 1)
    group = to // (far * seqs)
    rest = to - group * (far * seqs)
    block = rest // seqs
    source = (block * near + group) * seqs + rest - block * seqs
    order = jnp.where(at == source, 1.0, 0.0).astype(bf16)
    wide = product(order, tokens_ref[...])
    scaled = (wide * gain_ref[...].astype(f32)).astype(bf16)
    column = 0
    for weight in (gate_ref, value_ref, key_ref, query_ref):
        size = weight.shape[1]
        sent_ref[:, column : column + size] = product(scaled, weight[...]).astype(bf16)
        column += size
    heads = step_ref.shape[0]
    steps = jnp.concatenate(
        [step_ref[...].astype(f32), jnp.zeros((LANES - heads, width), f32)], axis=0
    ).astype(bf16)
    steps = lax.dot_general(
        scaled, steps, (((1,), (1,)), ((), ())), preferred_element_type=f32
    )
    squares = jnp.sum(wide * wide, axis=1, keepdims=True)
    high = squares.astype(bf16).astype(f32)
    lane = lax.broadcasted_iota(jnp.int32, (batch, LANES), 1)
    steps = jnp.where(lane == heads, high, jnp.where(lane == heads + 1, squares - high, steps))
    sent_ref[:, column:] = steps.astype(bf16)
    rows_ref[...] = wide.astype(bf16)


def project(tokens, norm_gain, w_gate, w_value, w_key, w_query, w_step, far, near):
    batch, width = tokens.shape
    columns = sum(w.shape[1] for w in (w_gate, w_value, w_key, w_query)) + LANES
    return pl.pallas_call(
        functools.partial(project_kernel, far, near, batch // (far * near)),
        out_shape=(
            jax.ShapeDtypeStruct((batch, columns), bf16),
            jax.ShapeDtypeStruct((batch, width), bf16),
        ),
        cost_estimate=pl.CostEstimate(
            flops=2 * batch * width * columns,
            bytes_accessed=2 * columns * (batch + width),
            transcendentals=0,
        ),
        name="project",
    )(tokens, norm_gain[None], w_gate, w_value, w_key, w_query, w_step.T)


def causal_conv(state_rows, newest, conv_weights):
    extended = jnp.concatenate([state_rows, newest[:, None]], axis=1)
    conv_sum = extended[:, 0] * conv_weights[0].astype(f32)
    for offset in range(1, conv_weights.shape[0]):
        conv_sum = conv_sum + extended[:, offset] * conv_weights[offset].astype(f32)
    return jax.nn.silu(conv_sum)


def product(left, right, out=f32):
    return jnp.dot(left, right, preferred_element_type=out)


def per_device(
    tokens,
    lengths,
    conv_state_x,
    conv_state_bc,
    ssm_state,
    norm_gain,
    w_gate,
    w_value,
    w_key,
    w_query,
    w_step,
    step_bias,
    decay_log,
    conv_x,
    conv_bc,
    inner_gain,
    w_out,
    mlp_gain,
    w_up,
    w_down,
):
    far, near = lax.axis_size("far"), lax.axis_size("near")
    head_count = w_step.shape[1]
    group_count = w_key.shape[1] // STATE
    per_group = head_count // group_count
    batch, width = tokens.shape
    model = width * far * near
    inner = w_gate.shape[1] * lax.axis_size("tp")
    seqs = batch // (far * near)

    sent, token_rows = project(
        tokens, norm_gain, w_gate, w_value, w_key, w_query, w_step, far, near
    )
    near_sum = scattered_sum(sent, "near").astype(bf16)
    mine = scattered_sum(near_sum, "far")

    hidden = w_up.shape[1] // near
    blocks = hidden // width
    extra = jnp.concatenate(
        [jnp.broadcast_to(mlp_gain[None], (8, width)), near_sum[:8, :width]], axis=0
    )
    packed = jnp.concatenate(
        [
            w_up.reshape(width, near, blocks, width).transpose(1, 2, 0, 3).reshape(near, -1, width),
            jnp.broadcast_to(w_out[None], (near, *w_out.shape)),
            token_rows.reshape(near, -1, width),
            jnp.broadcast_to(extra[None], (near, *extra.shape)),
        ],
        axis=1,
    )
    here = lax.axis_index("near")
    swapped = in_place(in_turn(packed, here), here)
    own_up = swapped[:, :hidden].reshape(near, blocks, width, width)
    own_up = own_up.transpose(0, 2, 1, 3).reshape(near * width, hidden)
    at = hidden + w_out.shape[0]
    own_out = swapped[:, hidden:at]
    near_tokens = swapped[:, at : at + batch // near].swapaxes(0, 1).reshape(-1, near * width)
    near_gain = swapped[:, at + batch // near].reshape(1, near * width).astype(f32)

    cuts, at = [], 0
    for size in (w_gate.shape[1], w_value.shape[1], w_key.shape[1], w_query.shape[1], head_count):
        cuts.append(mine[:, at : at + size])
        at += size
    gate_raw, value_raw, key_raw, query_raw, step_raw = cuts
    squares = jnp.sum(mine[:, at:], axis=1, keepdims=True)
    inverse = lax.rsqrt(squares / model + epsilon)

    row_live = (
        jnp.arange(CONV_WIDTH - 1, dtype=jnp.int32)[None, :] >= CONV_WIDTH - 1 - lengths[:, None]
    ).astype(f32)
    live_x = conv_state_x.astype(f32) * row_live[:, :, None]
    live_bc = conv_state_bc.astype(f32) * row_live[:, :, None, None]
    mixed_values = causal_conv(live_x, value_raw * inverse, conv_x).reshape(
        seqs, head_count, HEAD_DIM
    )
    key_query = causal_conv(
        live_bc, jnp.stack([key_raw * inverse, query_raw * inverse], axis=1), conv_bc
    )
    key_heads = jnp.repeat(key_query[:, 0].reshape(seqs, group_count, STATE), per_group, axis=1)
    query_heads = jnp.repeat(key_query[:, 1].reshape(seqs, group_count, STATE), per_group, axis=1)
    step_size = jax.nn.softplus(step_raw * inverse + step_bias)
    decay = jnp.exp(-jnp.exp(decay_log) * step_size)
    fed = step_size[:, :, None] * mixed_values
    overlap = jnp.sum(key_heads * query_heads, axis=2)
    mixer_y = (
        decay[:, :, None] * jnp.sum(ssm_state * query_heads[:, :, None, :], axis=3)
        + fed * overlap[:, :, None]
    ).reshape(seqs, head_count * HEAD_DIM)
    gated_rows = mixer_y * jax.nn.silu(gate_raw * inverse)
    gated_low = (gated_rows * inner_gain.astype(f32)).astype(bf16)
    gated_low, old_state = lax.optimization_barrier((gated_low, ssm_state))
    next_state = old_state * decay[:, :, None, None] + fed[:, :, :, None] * key_heads[:, :, None, :]
    picks = [here == i for i in range(near)]
    own_up, own_out, near_gain, near_tokens, next_state, picks = lax.optimization_barrier(
        (own_up, own_out, near_gain, near_tokens, next_state, picks)
    )

    all_low = from_everyone(gated_low, "far")
    all_low = all_low.reshape(far * seqs, -1)
    ungained = all_low.astype(f32) / inner_gain.astype(f32)
    gated_squares = hi_lo(jnp.sum(ungained * ungained, axis=1, keepdims=True))
    out_part = [product(all_low, own_out[i], bf16) for i in range(near)]
    shared = from_everyone(jnp.concatenate([*out_part, gated_squares], axis=1), "tp")
    shared = shared.astype(f32).sum(axis=0)
    gated_total = jnp.sum(shared[:, near * width :], axis=1, keepdims=True)
    residual = (
        near_tokens.astype(f32)
        + shared[:, : near * width] * lax.rsqrt(gated_total / inner + epsilon)
    ).astype(bf16)

    residual = from_everyone(residual, "near")
    residual = residual.reshape(batch, near * width)
    residual_wide = residual.astype(f32)
    hidden_low = (residual_wide * near_gain).astype(bf16)
    row_squares = jnp.sum(residual_wide * residual_wide, axis=1)
    chunk = batch // far
    up_part = product(hidden_low, own_up, bf16).reshape(far, chunk, blocks, width).swapaxes(1, 2)
    high = row_squares.astype(bf16)
    low = (row_squares - high.astype(f32)).astype(bf16)
    squares = jnp.concatenate([high.reshape(far, 1, chunk), low.reshape(far, 1, chunk)], axis=2)
    squares = jnp.pad(squares, ((0, 0), (0, 7), (0, width - 2 * chunk)))
    up_part = jnp.concatenate([up_part.reshape(far, blocks * chunk, width), squares], axis=1)
    own_rows = residual[:, :width]
    for i in range(1, near):
        own_rows = jnp.where(picks[i], residual[:, i * width : (i + 1) * width], own_rows)
    up_part, own_rows = lax.optimization_barrier((up_part, own_rows))
    up_mine = lax.all_to_all(up_part, "far", 0, 0, tiled=True)
    up_mine = up_mine.astype(f32).sum(axis=0)
    own_down = in_turn(w_down.reshape(near, hidden, width), here)
    up_share = up_mine[: blocks * chunk].reshape(blocks, chunk, width)
    square_share = up_mine[blocks * chunk]
    square_share = (square_share[:chunk] + square_share[chunk : 2 * chunk])[:, None]
    active = jnp.square(jax.nn.relu(up_share * lax.rsqrt(square_share / model + epsilon)))
    active = active.astype(bf16).swapaxes(0, 1).reshape(chunk, hidden)
    active = from_everyone(active, "far")
    active = active.reshape(batch, hidden)
    down_part = in_place([product(active, piece, bf16) for piece in own_down], here)
    down_sum = lax.all_to_all(down_part, "near", 0, 0, tiled=True).astype(f32).sum(axis=0)
    down_sum = from_everyone(down_sum.astype(bf16), "tp").astype(f32).sum(axis=0)
    finished = (own_rows.astype(f32) + down_sum).astype(bf16).reshape(near, far, seqs, width)
    return (finished.swapaxes(0, 1).reshape(batch, width), next_state)


def solution(mesh):
    kv = mesh.shape["kv"]
    near = NEAR if kv % NEAR == 0 else 1
    names = ("grp", "far", "near", "tp")
    split = Mesh(mesh.devices.reshape(mesh.shape["grp"], kv // near, near, mesh.shape["tp"]), names)
    kv = ("far", "near")
    seq = ("grp", "far", "near")
    return jax.shard_map(
        per_device,
        mesh=split,
        in_specs=(
            P("grp", kv),
            P(seq),
            P(seq, None, "tp"),
            P(seq, None, None, "tp"),
            P(seq, "tp", None, None),
            P(kv),
            P(kv, "tp"),
            P(kv, "tp"),
            P(kv, "tp"),
            P(kv, "tp"),
            P(kv, "tp"),
            P("tp"),
            P("tp"),
            P(None, "tp"),
            P(None, None, "tp"),
            P("tp"),
            P("tp", kv),
            P(kv),
            P(kv, "tp"),
            P("tp", kv),
        ),
        out_specs=(P("grp", kv), P(seq, "tp", None, None)),
        check_vma=False,
    )
```

```python
import functools

import jax
import jax.numpy as jnp
from jax import lax
from jax.experimental import pallas as pl
from jax.sharding import Mesh, PartitionSpec as P


HEAD_DIM = 64
STATE = 128
CONV_WIDTH = 4
LANES = 128
NEAR = 4

epsilon = 1e-06
f32, bf16 = jnp.float32, jnp.bfloat16


def scattered_sum(rows, along):
    size = lax.axis_size(along)
    parts = rows.reshape(size, -1, rows.shape[1])
    return lax.all_to_all(parts, along, 0, 0, tiled=True).astype(f32).sum(axis=0)


def from_everyone(shard, along):
    copies = jnp.broadcast_to(shard, (lax.axis_size(along), *shard.shape))
    return lax.all_to_all(copies, along, 0, 0, tiled=True)


def in_turn(packed, here):
    near = packed.shape[0]
    pieces = []
    for step in range(near):
        piece = lax.dynamic_index_in_dim(packed, here ^ step, keepdims=False)
        if step:
            piece = lax.ppermute(piece, "near", [(i, i ^ step) for i in range(near)])
        pieces.append(piece)
    return pieces


def in_place(pieces, here):
    pieces = jnp.stack(pieces)
    return jnp.stack(
        [lax.dynamic_index_in_dim(pieces, here ^ i, keepdims=False) for i in range(len(pieces))]
    )


def hi_lo(column):
    hi = column.astype(bf16)
    lo = (column - hi.astype(f32)).astype(bf16)
    lane = lax.broadcasted_iota(jnp.int32, (column.shape[0], LANES), 1)
    return jnp.where(lane == 0, hi, jnp.where(lane == 1, lo, jnp.zeros((), bf16)))


def project_kernel(
    far, near, seqs, tokens_ref, gain_ref, gate_ref, value_ref, key_ref, query_ref, step_ref, sent_ref, rows_ref
):
    batch, width = tokens_ref.shape
    to = lax.broadcasted_iota(jnp.int32, (batch, batch), 0)
    at = lax.broadcasted_iota(jnp.int32, (batch, batch), 1)
    group = to // (far * seqs)
    rest = to - group * (far * seqs)
    block = rest // seqs
    source = (block * near + group) * seqs + rest - block * seqs
    order = jnp.where(at == source, 1.0, 0.0).astype(bf16)
    wide = product(order, tokens_ref[...])
    scaled = (wide * gain_ref[...].astype(f32)).astype(bf16)
    column = 0
    for weight in (gate_ref, value_ref, key_ref, query_ref):
        size = weight.shape[1]
        sent_ref[:, column : column + size] = product(scaled, weight[...]).astype(bf16)
        column += size
    heads = step_ref.shape[0]
    steps = jnp.concatenate(
        [step_ref[...].astype(f32), jnp.zeros((LANES - heads, width), f32)], axis=0
    ).astype(bf16)
    steps = lax.dot_general(
        scaled, steps, (((1,), (1,)), ((), ())), preferred_element_type=f32
    )
    squares = jnp.sum(wide * wide, axis=1, keepdims=True)
    high = squares.astype(bf16).astype(f32)
    lane = lax.broadcasted_iota(jnp.int32, (batch, LANES), 1)
    steps = jnp.where(lane == heads, high, jnp.where(lane == heads + 1, squares - high, steps))
    sent_ref[:, column:] = steps.astype(bf16)
    rows_ref[...] = wide.astype(bf16)


def project(tokens, norm_gain, w_gate, w_value, w_key, w_query, w_step, far, near):
    batch, width = tokens.shape
    columns = sum(w.shape[1] for w in (w_gate, w_value, w_key, w_query)) + LANES
    return pl.pallas_call(
        functools.partial(project_kernel, far, near, batch // (far * near)),
        out_shape=(
            jax.ShapeDtypeStruct((batch, columns), bf16),
            jax.ShapeDtypeStruct((batch, width), bf16),
        ),
        cost_estimate=pl.CostEstimate(
            flops=2 * batch * width * columns,
            bytes_accessed=2 * columns * (batch + width),
            transcendentals=0,
        ),
        name="project",
    )(tokens, norm_gain[None], w_gate, w_value, w_key, w_query, w_step.T)


def causal_conv(state_rows, newest, conv_weights):
    extended = jnp.concatenate([state_rows, newest[:, None]], axis=1)
    conv_sum = extended[:, 0] * conv_weights[0].astype(f32)
    for offset in range(1, conv_weights.shape[0]):
        conv_sum = conv_sum + extended[:, offset] * conv_weights[offset].astype(f32)
    return jax.nn.silu(conv_sum)


def product(left, right, out=f32):
    return jnp.dot(left, right, preferred_element_type=out)


def per_device(
    tokens,
    lengths,
    conv_state_x,
    conv_state_bc,
    ssm_state,
    norm_gain,
    w_gate,
    w_value,
    w_key,
    w_query,
    w_step,
    step_bias,
    decay_log,
    conv_x,
    conv_bc,
    inner_gain,
    w_out,
    mlp_gain,
    w_up,
    w_down,
):
    far, near = lax.axis_size("far"), lax.axis_size("near")
    head_count = w_step.shape[1]
    group_count = w_key.shape[1] // STATE
    per_group = head_count // group_count
    batch, width = tokens.shape
    model = width * far * near
    inner = w_gate.shape[1] * lax.axis_size("tp")
    seqs = batch // (far * near)

    sent, token_rows = project(
        tokens, norm_gain, w_gate, w_value, w_key, w_query, w_step, far, near
    )
    near_sum = scattered_sum(sent, "near").astype(bf16)
    mine = scattered_sum(near_sum, "far")

    hidden = w_up.shape[1] // near
    blocks = hidden // width
    extra = jnp.concatenate(
        [jnp.broadcast_to(mlp_gain[None], (8, width)), near_sum[:8, :width]], axis=0
    )
    packed = jnp.concatenate(
        [
            w_up.reshape(width, near, blocks, width).transpose(1, 2, 0, 3).reshape(near, -1, width),
            jnp.broadcast_to(w_out[None], (near, *w_out.shape)),
            token_rows.reshape(near, -1, width),
            jnp.broadcast_to(extra[None], (near, *extra.shape)),
        ],
        axis=1,
    )
    here = lax.axis_index("near")
    swapped = in_place(in_turn(packed, here), here)
    own_up = swapped[:, :hidden].reshape(near, blocks, width, width)
    own_up = own_up.transpose(0, 2, 1, 3).reshape(near * width, hidden)
    at = hidden + w_out.shape[0]
    own_out = swapped[:, hidden:at]
    near_tokens = swapped[:, at : at + batch // near].swapaxes(0, 1).reshape(-1, near * width)
    near_gain = swapped[:, at + batch // near].reshape(1, near * width).astype(f32)

    cuts, at = [], 0
    for size in (w_gate.shape[1], w_value.shape[1], w_key.shape[1], w_query.shape[1], head_count):
        cuts.append(mine[:, at : at + size])
        at += size
    gate_raw, value_raw, key_raw, query_raw, step_raw = cuts
    squares = jnp.sum(mine[:, at:], axis=1, keepdims=True)
    inverse = lax.rsqrt(squares / model + epsilon)

    row_live = (
        jnp.arange(CONV_WIDTH - 1, dtype=jnp.int32)[None, :] >= CONV_WIDTH - 1 - lengths[:, None]
    ).astype(f32)
    live_x = conv_state_x.astype(f32) * row_live[:, :, None]
    live_bc = conv_state_bc.astype(f32) * row_live[:, :, None, None]
    mixed_values = causal_conv(live_x, value_raw * inverse, conv_x).reshape(
        seqs, head_count, HEAD_DIM
    )
    key_query = causal_conv(
        live_bc, jnp.stack([key_raw * inverse, query_raw * inverse], axis=1), conv_bc
    )
    key_heads = jnp.repeat(key_query[:, 0].reshape(seqs, group_count, STATE), per_group, axis=1)
    query_heads = jnp.repeat(key_query[:, 1].reshape(seqs, group_count, STATE), per_group, axis=1)
    step_size = jax.nn.softplus(step_raw * inverse + step_bias)
    decay = jnp.exp(-jnp.exp(decay_log) * step_size)
    fed = step_size[:, :, None] * mixed_values
    overlap = jnp.sum(key_heads * query_heads, axis=2)
    mixer_y = (
        decay[:, :, None] * jnp.sum(ssm_state * query_heads[:, :, None, :], axis=3)
        + fed * overlap[:, :, None]
    ).reshape(seqs, head_count * HEAD_DIM)
    gated_rows = mixer_y * jax.nn.silu(gate_raw * inverse)
    gated_low = (gated_rows * inner_gain.astype(f32)).astype(bf16)
    gated_low, old_state = lax.optimization_barrier((gated_low, ssm_state))
    added = fed[:, :, :, None] * key_heads[:, :, None, :]
    next_state = old_state * decay[:, :, None, None] + added
    picks = [here == i for i in range(near)]
    own_up, own_out, near_gain, near_tokens, picks = lax.optimization_barrier(
        (own_up, own_out, near_gain, near_tokens, picks)
    )

    all_low = from_everyone(gated_low, "far")
    all_low = all_low.reshape(far * seqs, -1)
    ungained = all_low.astype(f32) / inner_gain.astype(f32)
    gated_squares = hi_lo(jnp.sum(ungained * ungained, axis=1, keepdims=True))
    out_part = [product(all_low, own_out[i], bf16) for i in range(near)]
    shared = from_everyone(jnp.concatenate([*out_part, gated_squares], axis=1), "tp")
    shared = shared.astype(f32).sum(axis=0)
    gated_total = jnp.sum(shared[:, near * width :], axis=1, keepdims=True)
    residual = (
        near_tokens.astype(f32)
        + shared[:, : near * width] * lax.rsqrt(gated_total / inner + epsilon)
    ).astype(bf16)

    residual = from_everyone(residual, "near")
    residual = residual.reshape(batch, near * width)
    residual_wide = residual.astype(f32)
    hidden_low = (residual_wide * near_gain).astype(bf16)
    row_squares = jnp.sum(residual_wide * residual_wide, axis=1)
    chunk = batch // far
    up_part = product(hidden_low, own_up, bf16).reshape(far, chunk, blocks, width).swapaxes(1, 2)
    high = row_squares.astype(bf16)
    low = (row_squares - high.astype(f32)).astype(bf16)
    squares = jnp.concatenate([high.reshape(far, 1, chunk), low.reshape(far, 1, chunk)], axis=2)
    squares = jnp.pad(squares, ((0, 0), (0, 7), (0, width - 2 * chunk)))
    up_part = jnp.concatenate([up_part.reshape(far, blocks * chunk, width), squares], axis=1)
    own_rows = residual[:, :width]
    for i in range(1, near):
        own_rows = jnp.where(picks[i], residual[:, i * width : (i + 1) * width], own_rows)
    up_part, own_rows = lax.optimization_barrier((up_part, own_rows))
    up_mine = lax.all_to_all(up_part, "far", 0, 0, tiled=True)
    up_mine = up_mine.astype(f32).sum(axis=0)
    own_down = in_turn(w_down.reshape(near, hidden, width), here)
    up_share = up_mine[: blocks * chunk].reshape(blocks, chunk, width)
    square_share = up_mine[blocks * chunk]
    square_share = (square_share[:chunk] + square_share[chunk : 2 * chunk])[:, None]
    active = jnp.square(jax.nn.relu(up_share * lax.rsqrt(square_share / model + epsilon)))
    active = active.astype(bf16).swapaxes(0, 1).reshape(chunk, hidden)
    active = from_everyone(active, "far")
    active = active.reshape(batch, hidden)
    down_part = in_place([product(active, piece, bf16) for piece in own_down], here)
    down_sum = lax.all_to_all(down_part, "near", 0, 0, tiled=True).astype(f32).sum(axis=0)
    down_sum = from_everyone(down_sum.astype(bf16), "tp").astype(f32).sum(axis=0)
    finished = (own_rows.astype(f32) + down_sum).astype(bf16).reshape(near, far, seqs, width)
    return (finished.swapaxes(0, 1).reshape(batch, width), next_state)


def solution(mesh):
    kv = mesh.shape["kv"]
    near = NEAR if kv % NEAR == 0 else 1
    names = ("grp", "far", "near", "tp")
    split = Mesh(mesh.devices.reshape(mesh.shape["grp"], kv // near, near, mesh.shape["tp"]), names)
    kv = ("far", "near")
    seq = ("grp", "far", "near")
    return jax.shard_map(
        per_device,
        mesh=split,
        in_specs=(
            P("grp", kv),
            P(seq),
            P(seq, None, "tp"),
            P(seq, None, None, "tp"),
            P(seq, "tp", None, None),
            P(kv),
            P(kv, "tp"),
            P(kv, "tp"),
            P(kv, "tp"),
            P(kv, "tp"),
            P(kv, "tp"),
            P("tp"),
            P("tp"),
            P(None, "tp"),
            P(None, None, "tp"),
            P("tp"),
            P("tp", kv),
            P(kv),
            P(kv, "tp"),
            P("tp", kv),
        ),
        out_specs=(P("grp", kv), P(seq, "tp", None, None)),
        check_vma=False,
    )
```
